512 devices in a mesh: sp: 64 (over z, y), tp: 8 (over x, core).
Axes of the slice: x: 4, y: 4, z: 16, core: 2. Of those that a mesh axis runs over, the one named last changes fastest.
Arguments:
- resid: bfloat16 [16384, 2048], P('sp', 'tp'), may hold values from -6 to 6
- queries: bfloat16 [16384, 1024], P('sp', 'tp'), may hold values from -6 to 6
- keys_values: bfloat16 [8, 16384, 128], P('tp', 'sp'), may hold values from -6 to 6
- cum_gate: float32 [16, 16384], P('tp', 'sp'), as said below
- out_weight: bfloat16 [1024, 2048], P(None, 'tp'), may hold values from -1.5 to 1.5
- norm_gain: float32 [2048], replicated, may hold values from 0.1 to 1.9
- gate_weight: bfloat16 [2048, 5632], P('sp', 'tp'), may hold values from -0.125 to 0.125
- up_weight: bfloat16 [2048, 5632], P('sp', 'tp'), may hold values from -0.125 to 0.125
- conv_kernel: float32 [3, 2, 5632], P(None, None, 'tp'), may hold values from -3.5 to 3.5
- down_weight: bfloat16 [5632, 2048], P('tp', 'sp'), may hold values from -0.078125 to 0.078125
Outputs:
- layer_out: bfloat16 [16384, 2048], P('sp', 'tp')
The draws below stay inside these ranges and needn't reach their ends.
Inputs may be any that keep to these rules, and one draw needn't show every extreme that they name: `cum_gate`: along positions each head's entries never increase.
All inputs are finite; a program needn't handle non-finite values.
Results may differ from the reference program's by a relative error of at most 0.015.
Values may be sent and summed in bfloat16 or wider, within the bound.
No kernel may reach another device: no remote copies, remote signals or barrier semaphores. Data moves between devices by JAX's collectives and lax.ppermute only.
A program may use at most 64 MiB of HBM per device.

```python
import math
import jax
import jax.numpy as jnp
from jax import lax

D = 2048
QUERY_HEAD_COUNT = 16
KV_HEADS = 8
HD = 64
FF = 5632
KSIZE = 3
TOK_DEV = 256
SEQUENCE_TOKENS = 16384


def draw_queries(key, part):
    drawn = jnp.clip(jax.random.normal(jax.random.fold_in(key, 1), (SEQUENCE_TOKENS, QUERY_HEAD_COUNT * HD), jnp.float32), -5.9, 5.9)
    return drawn.astype(jnp.bfloat16)


def draw_keys_values(key, part):
    drawn = jnp.clip(jax.random.normal(jax.random.fold_in(key, 2), (KV_HEADS, SEQUENCE_TOKENS, 2 * HD), jnp.float32), -5.9, 5.9)
    return drawn.astype(jnp.bfloat16)


def draw_cum_gate(key, part):
    order = jax.random.permutation(jax.random.fold_in(key, 11), QUERY_HEAD_COUNT)
    quick_decay_heads = order < QUERY_HEAD_COUNT // 2
    fast_rate = jnp.exp(jax.random.uniform(jax.random.fold_in(key, 12), (QUERY_HEAD_COUNT,), jnp.float32, jnp.log(1.0 / 100.0), jnp.log(1.0 / 30.0)))
    slow_total = jnp.exp(jax.random.uniform(jax.random.fold_in(key, 13), (QUERY_HEAD_COUNT,), jnp.float32, jnp.log(0.3), jnp.log(0.8)))
    baseline_decay = jnp.where(quick_decay_heads, fast_rate, slow_total / SEQUENCE_TOKENS)
    jitter_amplitude = jnp.exp(jax.random.uniform(jax.random.fold_in(key, 14), (QUERY_HEAD_COUNT, SEQUENCE_TOKENS), jnp.float32, jnp.log(0.5), jnp.log(2.0)))
    block_multiplier = jnp.exp(jax.random.uniform(jax.random.fold_in(key, 15), (QUERY_HEAD_COUNT, SEQUENCE_TOKENS // TOK_DEV), jnp.float32, jnp.log(0.5), jnp.log(2.0)))
    block_multiplier = jnp.repeat(block_multiplier, TOK_DEV, axis=1)
    spike_locations = jax.random.randint(jax.random.fold_in(key, 16), (2,), 1, SEQUENCE_TOKENS)
    token_places = jnp.arange(SEQUENCE_TOKENS)
    spike_active = (token_places[:, None] == spike_locations[None, :]).any(axis=1)
    spike_penalty = jax.random.uniform(jax.random.fold_in(key, 17), (QUERY_HEAD_COUNT, SEQUENCE_TOKENS), jnp.float32, 0.2, 0.4)
    spike_addend = jnp.where(spike_active[None, :] & jnp.logical_not(quick_decay_heads)[:, None], jnp.log(1.0 - spike_penalty), 0.0)
    gate_logarithm = -baseline_decay[:, None] * jitter_amplitude * block_multiplier + spike_addend
    return jnp.cumsum(gate_logarithm, axis=1).astype(jnp.float32)


def steps_of(own_key, shape, pieces, low, high):
    gain, own = 1.0, jax.random.fold_in(own_key, 6)
    for axis_at, parts in pieces:
        steps = jnp.exp(jax.random.uniform(jax.random.fold_in(own, axis_at), (parts,), jnp.float32, low / len(pieces), high / len(pieces)))
        gain = gain * jnp.repeat(steps, shape[axis_at] // parts).reshape([-1 if axis == axis_at else 1 for axis in range(len(shape))])
    return gain


def gaussian(stream_key, extent, width, limit, pieces=(), held_as=jnp.bfloat16):
    loudness = steps_of(stream_key, extent, pieces, -0.22, 0.18) if pieces else 1.0
    array = jax.random.normal(stream_key, extent, jnp.float32) * width * loudness
    return jnp.minimum(jnp.maximum(array, -limit), limit).astype(held_as)


def setup_inputs(seed: int = 0) -> dict:
    splits = jax.random.split(jax.random.key(seed), 11)
    resid = gaussian(splits[0], (SEQUENCE_TOKENS, D), 1.0, 6.0, ((0, 64), (1, 8)))
    queries = draw_queries(jax.random.fold_in(splits[10], 71), 0)
    keys_values = draw_keys_values(jax.random.fold_in(splits[10], 71), 0)
    cum_gate = draw_cum_gate(jax.random.fold_in(splits[10], 71), 0)
    out_weight = gaussian(splits[4], (QUERY_HEAD_COUNT * HD, D), 0.25, 1.5, ((1, 8),))
    norm_gain = jnp.clip(1.0 + 0.18 * jax.random.normal(splits[5], (D,), jnp.float32), 0.1, 1.9)
    gate_weight = gaussian(splits[6], (D, FF), D ** -0.5, 0.125, ((0, 64), (1, 8)))
    up_weight = gaussian(splits[7], (D, FF), D ** -0.5, 0.125, ((0, 64), (1, 8)))
    conv_kernel = gaussian(splits[8], (KSIZE, 2, FF), KSIZE ** -0.5, 3.5, ((2, 8),), jnp.float32)
    down_weight = gaussian(splits[9], (FF, D), FF ** -0.5, 0.078125, ((0, 8), (1, 64)))
    return dict(resid=resid, queries=queries, keys_values=keys_values, cum_gate=cum_gate, out_weight=out_weight, norm_gain=norm_gain, gate_weight=gate_weight, up_weight=up_weight, conv_kernel=conv_kernel, down_weight=down_weight)


norm_eps = 1e-06

def reference(resid, queries, keys_values, cum_gate, out_weight, norm_gain, gate_weight, up_weight, conv_kernel, down_weight):
    group_size = QUERY_HEAD_COUNT // KV_HEADS
    score_scale = HD ** (-0.5)
    query_rows = math.gcd(SEQUENCE_TOKENS, 512)
    block_count = SEQUENCE_TOKENS // query_rows
    key_positions = jnp.arange(SEQUENCE_TOKENS, dtype=jnp.int32)

    def one_item(item_index):
        head = item_index // block_count
        block = item_index % block_count
        first = (block * query_rows).astype(jnp.int32)
        query_part = lax.dynamic_slice(queries, (first, (head * HD).astype(jnp.int32)), (query_rows, HD))
        pair = lax.dynamic_index_in_dim(keys_values, (head // group_size).astype(jnp.int32), 0, keepdims=False)
        key_rows = pair[:, :HD]
        value_rows = pair[:, HD:]
        head_gates = lax.dynamic_index_in_dim(cum_gate, head.astype(jnp.int32), 0, keepdims=False)
        query_gates = lax.dynamic_slice_in_dim(head_gates, first, query_rows)
        scores = jnp.dot(query_part, key_rows.T, preferred_element_type=jnp.float32) * score_scale
        scores = scores + query_gates[:, None] - head_gates[None, :]
        query_positions = first + jnp.arange(query_rows, dtype=jnp.int32)
        visible = key_positions[None, :] <= query_positions[:, None]
        row_max = lax.optimization_barrier(jnp.max(jnp.where(visible, scores, -jnp.inf), axis=1))
        weights = jnp.where(visible, jnp.exp(scores - row_max[:, None]), 0.0)
        row_sum = lax.optimization_barrier(jnp.sum(weights, axis=1))
        result = jnp.dot(weights.astype(jnp.bfloat16), value_rows, preferred_element_type=jnp.float32)
        return result / row_sum[:, None]
    heads_out = lax.map(one_item, jnp.arange(QUERY_HEAD_COUNT * block_count, dtype=jnp.int32))
    heads_out = heads_out.reshape(QUERY_HEAD_COUNT, block_count, query_rows, HD).transpose(1, 2, 0, 3)
    attn = heads_out.reshape(SEQUENCE_TOKENS, QUERY_HEAD_COUNT * HD).astype(jnp.bfloat16)
    middle = (resid.astype(jnp.float32) + jnp.dot(attn, out_weight, preferred_element_type=jnp.float32)).astype(jnp.bfloat16)
    middle_f32 = middle.astype(jnp.float32)
    inverse = lax.rsqrt(lax.optimization_barrier(jnp.mean(middle_f32 * middle_f32, axis=1, keepdims=True)) + norm_eps)
    normed = (middle_f32 * inverse * norm_gain).astype(jnp.bfloat16)
    pre_gate = jnp.dot(normed, gate_weight, preferred_element_type=jnp.float32).astype(jnp.bfloat16)
    pre_up = jnp.dot(normed, up_weight, preferred_element_type=jnp.float32).astype(jnp.bfloat16)
    joined = jnp.concatenate([pre_gate, pre_up], axis=1).astype(jnp.float32)
    padded = jnp.concatenate([jnp.zeros((KSIZE - 1, 2 * FF), jnp.float32), joined], axis=0)
    kernel = conv_kernel.reshape(KSIZE, 2 * FF)
    mixed = jnp.zeros((SEQUENCE_TOKENS, 2 * FF), jnp.float32)
    for offset in range(KSIZE):
        mixed = mixed + kernel[offset][None, :] * padded[offset:offset + SEQUENCE_TOKENS]
    hidden = (jax.nn.silu(mixed[:, :FF]) * mixed[:, FF:]).astype(jnp.bfloat16)
    channel_out = jnp.dot(hidden, down_weight, preferred_element_type=jnp.float32)
    return (middle_f32 + channel_out).astype(jnp.bfloat16)
```

```python
import functools

import jax
import jax.numpy as jnp
from jax import lax
from jax.experimental import pallas as pl
from jax.experimental.pallas import tpu as pltpu
from jax.sharding import Mesh
from jax.sharding import PartitionSpec as P

Z = ("zh", "zl")
Y = ("yh", "yl")
SP = Z + Y
TP = ("x", "c")
NORM_EPS = 1e-06
HALO = 16
MASKED = -1e30
F32 = jnp.float32
BF16 = jnp.bfloat16


def shifted(value, axis, by):
    size = lax.axis_size(axis)
    return lax.ppermute(value, axis, [(i, (i + by) % size) for i in range(size)])


def exchanged(value, axis):
    return lax.all_to_all(value, axis, 0, 0, tiled=True)


def spread(value, axis):
    size = lax.axis_size(axis)
    return exchanged(jnp.broadcast_to(value[None], (size, *value.shape)), axis)


def three_parts(value):
    high = lax.reduce_precision(value, 8, 7)
    rest = value - high
    middle = lax.reduce_precision(rest, 8, 7)
    low = lax.reduce_precision(rest - middle, 8, 7)
    return high, middle, low


def split3(value):
    high = value.astype(BF16)
    rest = value - high.astype(F32)
    middle = rest.astype(BF16)
    low = (rest - middle.astype(F32)).astype(BF16)
    return high, middle, low


def attend_kernel(at_ref, gate_ref, q_ref, own_ref, next_ref, far_a_ref, far_b_ref, last_ref,
                  out_ref, qa, ka, va, norm_out, lse_rows, lse_dense, *, rows, block):
    zh, zl, y = at_ref[0], at_ref[1], at_ref[2]
    z = 4 * zh + zl
    lane = lax.broadcasted_iota(jnp.int32, (1, 128), 1)
    group = rows - HALO

    def put_queries(start, piece):
        x = piece.astype(F32) * 0.125
        for head in range(2):
            part = x if head == 0 else pltpu.roll(x, 64, 1)
            first = 64 + 3 * head
            ones = jnp.where((lane >= first) & (lane < first + 3), 1.0, 0.0)
            both = jnp.where(lane < 64, part, ones)
            qa[pl.ds(head * rows + start, piece.shape[0]), :] = both.astype(BF16)

    put_queries(0, q_ref[0, 0:HALO, :])
    for i in range(4):
        put_queries(HALO + 256 * i, q_ref[i, HALO:HALO + 256, :])

    part_row = lax.broadcasted_iota(jnp.int32, (16, 256), 0)

    def put_keys(chunk, d, piece):
        cols = pl.ds(256 * d, 256)
        ka[chunk, 0:64, cols] = piece[0:64, :]
        g = piece[64:80, :].astype(F32)
        bias = []
        for head in range(2):
            total = g[3 * head:3 * head + 1, :] + g[3 * head + 1:3 * head + 2, :]
            bias.append(gate_ref[head] - (total + g[3 * head + 2:3 * head + 3, :]))
        b = jnp.where(part_row < 3, bias[0], bias[1])
        which = jnp.where(part_row < 3, part_row, part_row - 3)
        high, middle, low = split3(b)
        pick = jnp.where(which == 0, high.astype(F32), jnp.where(which == 1, middle.astype(F32), low.astype(F32)))
        ka[chunk, 64:80, cols] = jnp.where(part_row < 6, pick, 0.0).astype(BF16)
        ka[chunk, 80:128, cols] = jnp.zeros((48, 256), BF16)
        va[chunk, 0:64, cols] = piece[80:144, :]
        va[chunk, 64:128, cols] = jnp.ones((64, 256), BF16)

    for chunk in range(4):
        far = far_a_ref[chunk] if chunk < 2 else far_b_ref[chunk - 2]
        pieces = (own_ref[chunk], next_ref[chunk], far, last_ref[chunk])
        for d in range(4):
            put_keys(chunk, d, pieces[d])

    key_lane = lax.broadcasted_iota(jnp.int32, (1, 1024), 1)
    key_d = key_lane // 256
    first_masked = jnp.maximum(zh - jnp.where(zl == 0, 1, 0), 0)

    def row_block(r, _):
        start = pl.multiple_of(r * block, block)
        q = qa[pl.ds(start, block), :]
        row = start + lax.broadcasted_iota(jnp.int32, (block, 1), 0)
        query_pos = z * group - HALO + jnp.where(row >= rows, row - rows, row)

        def step(masked, chunk, state):
            top, acc = state
            s = lax.dot_general(q, ka[chunk], (((1,), (0,)), ((), ())), preferred_element_type=F32)
            if masked:
                turn = zl + key_d
                key_z = 4 * chunk + jnp.where(turn >= 4, turn - 4, turn)
                key_pos = key_z * group + y * 256 + (key_lane - 256 * key_d)
                s = jnp.where(query_pos >= key_pos, s, MASKED)
            new_top = jnp.maximum(top, jnp.max(s, axis=1, keepdims=True))
            p = jnp.exp(s - new_top).astype(BF16)
            more = lax.dot_general(p, va[chunk], (((1,), (1,)), ((), ())), preferred_element_type=F32)
            return new_top, acc * jnp.exp(top - new_top) + more

        state = (jnp.full((block, 1), MASKED, F32), jnp.zeros((block, 128), F32))
        state = lax.fori_loop(0, first_masked, functools.partial(step, False), state)
        top, acc = lax.fori_loop(first_masked, zh + 1, functools.partial(step, True), state)
        total = acc[:, 64:65]
        gate = jnp.where(row >= rows, gate_ref[1], gate_ref[0])
        norm_out[pl.ds(start, block), :] = acc / total
        lse_rows[pl.ds(start, block), :] = jnp.broadcast_to(top + jnp.log(total) - gate, (block, 128))
        return 0

    lax.fori_loop(0, 2 * rows // block, row_block, 0)
    tail = lse_rows.shape[0] - 2 * rows
    lse_rows[pl.ds(2 * rows, tail), :] = jnp.zeros((tail, 128), F32)
    lse_dense[...] = jnp.zeros(lse_dense.shape, F32)
    diagonal = lax.broadcasted_iota(jnp.int32, (128, 128), 0) == lax.broadcasted_iota(jnp.int32, (128, 128), 1)
    pair_rows = HALO + 512
    for pair in range(2):
        a = norm_out[pl.ds(512 * pair, pair_rows), :]
        b = norm_out[pl.ds(rows + 512 * pair, pair_rows), :]
        joined = jnp.where(lane < 64, a, pltpu.roll(b, 64, 1)).astype(BF16)
        for head in range(2):
            for t in range(5):
                tile = lse_rows[pl.ds(head * rows + 512 * pair + 128 * t, 128), :]
                lse_dense[pl.ds(5 * head + t, 1), :] = jnp.sum(jnp.where(diagonal, tile, 0.0), axis=0, keepdims=True)
        parts = split3(lse_dense[...])
        for i in range(2):
            out_ref[2 * pair + i, 0:pair_rows, :] = joined
            for k in range(3):
                out_ref[2 * pair + i, pair_rows + 16 * k:pair_rows + 16 * (k + 1), :] = parts[k]


def attend(at, gate, queries, own, nxt, far_a, far_b, last):
    rows = HALO + 1024
    pair_rows = HALO + 512
    smem = pl.BlockSpec(memory_space=pltpu.SMEM)
    vmem = pl.BlockSpec(memory_space=pltpu.VMEM)
    return pl.pallas_call(
        functools.partial(attend_kernel, rows=rows, block=416),
        out_shape=jax.ShapeDtypeStruct((4, pair_rows + 48, 128), BF16),
        in_specs=[smem, smem] + [vmem] * 6,
        out_specs=vmem,
        scratch_shapes=[
            pltpu.VMEM((2 * rows, 128), BF16),
            pltpu.VMEM((4, 128, 1024), BF16),
            pltpu.VMEM((4, 128, 1024), BF16),
            pltpu.VMEM((2 * rows, 128), F32),
            pltpu.VMEM((2 * rows + 112, 128), F32),
            pltpu.VMEM((16, 128), F32),
        ],
        cost_estimate=pl.CostEstimate(flops=8 * 10**9, bytes_accessed=4 * 2**20, transcendentals=8 * 10**6),
        name="attend",
    )(at, gate, queries, own, nxt, far_a, far_b, last)


def merge_kernel(in_ref, out_ref):
    pair_rows = HALO + 512
    logs = []
    for i in range(4):
        parts = [in_ref[i, pair_rows + 16 * k:pair_rows + 16 * (k + 1), :].astype(F32) for k in range(3)]
        logs.append(parts[0] + parts[1] + parts[2])
    top = jnp.maximum(jnp.maximum(logs[0], logs[1]), jnp.maximum(logs[2], logs[3]))
    weights = [jnp.exp(v - top) for v in logs]
    total = weights[0] + weights[1] + weights[2] + weights[3]
    shares = [w / total for w in weights]
    lane = lax.broadcasted_iota(jnp.int32, (1, 128), 1)
    for t in range(5):
        size = 128 if t < 4 else pair_rows - 512
        diagonal = lax.broadcasted_iota(jnp.int32, (size, 128), 0) == lax.broadcasted_iota(jnp.int32, (size, 128), 1)
        acc = jnp.zeros((size, 128), F32)
        for i in range(4):
            cols = [
                jnp.sum(jnp.where(diagonal, shares[i][5 * head + t:5 * head + t + 1, :], 0.0), axis=1, keepdims=True)
                for head in range(2)
            ]
            share = jnp.where(lane < 64, cols[0], cols[1])
            acc = acc + share * in_ref[i, 128 * t:128 * t + size, :].astype(F32)
        out_ref[128 * t:128 * t + size, :] = acc.astype(BF16)


def merge(pieces):
    vmem = pl.BlockSpec(memory_space=pltpu.VMEM)
    return pl.pallas_call(
        merge_kernel,
        out_shape=jax.ShapeDtypeStruct((HALO + 512, 128), BF16),
        in_specs=[vmem],
        out_specs=vmem,
        cost_estimate=pl.CostEstimate(flops=10**8, bytes_accessed=2**20, transcendentals=10**4),
        name="merge",
    )(pieces)


def feed_kernel(at_ref, attn_ref, wide_ref, gain_ref, conv_ref, w_ref, part_ref, mid_out_ref,
                af, mid, normed, wg, wu, wd, sems):
    copies = []
    for k, dst in enumerate((wg, wu, wd)):
        copy = pltpu.make_async_copy(w_ref.at[:, :, k], dst, sems.at[k])
        copy.start()
        copies.append(copy)
    is_first, half, block = at_ref[3], at_ref[4], at_ref[5]
    rows = HALO + 512
    for x in range(4):
        for c in range(2):
            af[:, 128 * (2 * x + c):128 * (2 * x + c + 1)] = attn_ref[c, x]
    a = af[...]
    square = jnp.zeros((rows, 1), F32)
    for x in range(4):
        for c in range(2):
            j = 2 * x + c
            branch = jnp.dot(a, wide_ref[c, x, 0:1024, :], preferred_element_type=F32)
            m = (branch + wide_ref[c, x, 1024:1024 + rows, :].astype(F32)).astype(BF16)
            mid[:, 256 * j:256 * (j + 1)] = m
            m = m.astype(F32)
            square = square + jnp.sum(m * m, axis=1, keepdims=True)
    inverse = lax.rsqrt(square * (1.0 / 2048) + NORM_EPS)
    for j in range(8):
        cols = slice(256 * j, 256 * (j + 1))
        normed[:, cols] = (mid[:, cols].astype(F32) * inverse * gain_ref[:, cols]).astype(BF16)
    mid_out_ref[...] = mid[pl.ds(pl.multiple_of(HALO + 256 * half, 16), 256), pl.ds(pl.multiple_of(256 * block, 256), 256)]
    n = normed[...]
    copies[0].wait()
    copies[1].wait()
    row = lax.broadcasted_iota(jnp.int32, (rows, 1), 0)
    keep = jnp.logical_not((row < HALO) & (is_first == 1))

    def mixed(weight, index):
        pre = jnp.dot(n, weight[...].reshape(2048, 352), preferred_element_type=F32).astype(BF16).astype(F32)
        pre = jnp.where(keep, pre, 0.0)
        total = jnp.zeros((512, 352), F32)
        for k in range(3):
            total = total + conv_ref[2 * k + index:2 * k + index + 1, :] * pre[HALO - 2 + k:HALO - 2 + k + 512]
        return total

    gate = mixed(wg, 0)
    up = mixed(wu, 1)
    hidden = (gate / (1.0 + jnp.exp(-gate)) * up).astype(BF16)
    copies[2].wait()
    down = wd[...].reshape(2048, 352)
    for x in range(4):
        for c in range(2):
            j = 2 * x + c
            part = lax.dot_general(hidden, down[256 * j:256 * (j + 1)], (((1,), (1,)), ((), ())), preferred_element_type=F32)
            part = part.astype(BF16)
            for p in range(2):
                part_ref[c, p, x] = part[256 * p:256 * (p + 1)]


def feed(at, attn, wide, gain, conv, weights):
    smem = pl.BlockSpec(memory_space=pltpu.SMEM)
    vmem = pl.BlockSpec(memory_space=pltpu.VMEM)
    rows = HALO + 512
    return pl.pallas_call(
        feed_kernel,
        out_shape=(
            jax.ShapeDtypeStruct((2, 2, 4, 256, 256), BF16),
            jax.ShapeDtypeStruct((256, 256), BF16),
        ),
        in_specs=[smem, vmem, vmem, vmem, vmem, pl.BlockSpec(memory_space=pl.ANY)],
        out_specs=(vmem, vmem),
        scratch_shapes=[
            pltpu.VMEM((rows, 1024), BF16),
            pltpu.VMEM((rows, 2048), BF16),
            pltpu.VMEM((rows, 2048), BF16),
            pltpu.VMEM((16, 4, 32, 352), BF16),
            pltpu.VMEM((16, 4, 32, 352), BF16),
            pltpu.VMEM((16, 4, 32, 352), BF16),
            pltpu.SemaphoreType.DMA((3,)),
        ],
        cost_estimate=pl.CostEstimate(flops=5 * 10**9, bytes_accessed=2**24, transcendentals=2 * 10**5),
        name="feed",
    )(at, attn, wide, gain, conv, weights)


def local(resid, queries, keys_values, cum_gate, out_weight, norm_gain, gate_weight, up_weight, conv_kernel, down_weight):
    zh, zl = lax.axis_index("zh"), lax.axis_index("zl")
    y, half = lax.axis_index(Y), lax.axis_index("yl")
    is_first = (lax.axis_index(SP) < 2).astype(jnp.int32)
    at = jnp.stack([zh, zl, y, is_first, half, lax.axis_index(TP)]).astype(jnp.int32)

    with jax.named_scope("weights"):
        three = jnp.stack([gate_weight, up_weight, down_weight.T])
        halves = jnp.moveaxis(three.reshape(3, 32, 2, 352), 2, 0)
        send = jnp.broadcast_to(halves[None], (2, 2, 3, 32, 352)).reshape(4, 3, 32, 352)
        rows_y = exchanged(send, Y)
        weights = lax.all_gather(rows_y, Z, axis=0, tiled=False)

    with jax.named_scope("keys"):
        turned = keys_values[0].T
        parts = three_parts(cum_gate)
        gates = jnp.stack(parts, axis=1).reshape(6, 256).astype(BF16)
        wire = jnp.concatenate([turned[:64], gates, jnp.zeros((10, 256), BF16), turned[64:]], axis=0)
        own = spread(wire, "zh")
        last = shifted(own, Z, 1)
        nxt = shifted(own, Z, -1)
        far_a = shifted(own[:2], Z, -2)
        far_b = shifted(own[2:], Z, 2)

    with jax.named_scope("halo"):
        tail = jnp.concatenate([queries[-HALO:], resid[-HALO:]], axis=1)
        before = shifted(tail, SP, 1)
    with jax.named_scope("queries"):
        group_q = spread(jnp.concatenate([before[:, :128], queries], axis=0), Y)
    with jax.named_scope("wide"):
        pair = spread(jnp.concatenate([before[:, 128:], resid], axis=0), "yl")
        pair = jnp.concatenate([pair[0], pair[1, HALO:]], axis=0)
        wide = spread(spread(jnp.concatenate([out_weight, pair], axis=0), "x"), "c")

    partial = attend(at, cum_gate[:, 0], group_q, own, nxt, far_a, far_b, last)
    with jax.named_scope("merge"):
        attn = merge(exchanged(partial, Y))
    with jax.named_scope("heads"):
        attn = spread(lax.all_gather(attn, "x", axis=0, tiled=False), "c")
    conv = lax.dynamic_slice_in_dim(conv_kernel.reshape(6, 704), half * 352, 352, 1)
    part, middle = feed(at, attn, wide, norm_gain.reshape(1, 2048), conv, weights)
    with jax.named_scope("sums"):
        cores = exchanged(part, "c").astype(F32)
        chip = (cores[0] + cores[1]).astype(BF16).reshape(8, 256, 256)
        pieces = exchanged(chip, ("yl", "x"))
        total = jnp.sum(pieces.astype(F32), axis=0)
    return (middle.astype(F32) + total).astype(BF16)


def solution(mesh):
    finer = Mesh(mesh.devices.reshape(4, 4, 2, 2, 4, 2), SP + TP)
    return jax.shard_map(
        local,
        mesh=finer,
        in_specs=(
            P(SP, TP),
            P(SP, TP),
            P(TP, SP, None),
            P(TP, SP),
            P(None, TP),
            P(),
            P(SP, TP),
            P(SP, TP),
            P(None, None, TP),
            P(TP, SP),
        ),
        out_specs=P(SP, TP),
        check_vma=False,
    )
```

```python
import functools

import jax
import jax.numpy as jnp
from jax import lax
from jax.experimental import pallas as pl
from jax.experimental.pallas import tpu as pltpu
from jax.sharding import Mesh
from jax.sharding import PartitionSpec as P


Z = ("zh", "zl")
Y = ("yh", "yl")
SP = Z + Y
TP = ("x", "c")
NORM_EPS = 1e-06
HALO = 16
MASKED = -1e30
F32 = jnp.float32
BF16 = jnp.bfloat16


def shifted(value, axis, by):
    size = lax.axis_size(axis)
    return lax.ppermute(value, axis, [(i, (i + by) % size) for i in range(size)])


def exchanged(value, axis):
    return lax.all_to_all(value, axis, 0, 0, tiled=True)


def spread(value, axis):
    size = lax.axis_size(axis)
    return exchanged(jnp.broadcast_to(value[None], (size, *value.shape)), axis)


def split3(value):
    high = value.astype(BF16)
    rest = value - high.astype(F32)
    middle = rest.astype(BF16)
    low = (rest - middle.astype(F32)).astype(BF16)
    return high, middle, low


def attend_kernel(at_ref, gate_ref, q_ref, own_ref, next_ref, far_a_ref, far_b_ref, last_ref,
                  out_ref, qa, ka, va, norm_out, lse_rows, lse_dense, *, rows, block):
    zh, zl, y = at_ref[0], at_ref[1], at_ref[2]
    z = 4 * zh + zl
    lane = lax.broadcasted_iota(jnp.int32, (1, 128), 1)
    group = rows - HALO

    def put_queries(start, piece):
        x = piece.astype(F32) * 0.125
        for head in range(2):
            part = x if head == 0 else pltpu.roll(x, 64, 1)
            first = 64 + 3 * head
            ones = jnp.where((lane >= first) & (lane < first + 3), 1.0, 0.0)
            both = jnp.where(lane < 64, part, ones)
            qa[pl.ds(head * rows + start, piece.shape[0]), :] = both.astype(BF16)

    put_queries(0, q_ref[0, 0:HALO, :])
    for i in range(4):
        put_queries(HALO + 256 * i, q_ref[i, HALO:HALO + 256, :])

    part_row = lax.broadcasted_iota(jnp.int32, (16, 256), 0)

    def put_keys(chunk, d, piece):
        cols = pl.ds(256 * d, 256)
        ka[chunk, 0:64, cols] = piece[0:64, :]
        g = piece[64:80, :].astype(F32)
        bias = []
        for head in range(2):
            total = g[3 * head:3 * head + 1, :] + g[3 * head + 1:3 * head + 2, :]
            bias.append(gate_ref[head] - (total + g[3 * head + 2:3 * head + 3, :]))
        b = jnp.where(part_row < 3, bias[0], bias[1])
        which = jnp.where(part_row < 3, part_row, part_row - 3)
        high, middle, low = split3(b)
        pick = jnp.where(which == 0, high.astype(F32), jnp.where(which == 1, middle.astype(F32), low.astype(F32)))
        ka[chunk, 64:80, cols] = jnp.where(part_row < 6, pick, 0.0).astype(BF16)
        ka[chunk, 80:128, cols] = jnp.zeros((48, 256), BF16)
        va[chunk, 0:64, cols] = piece[80:144, :]
        va[chunk, 64:128, cols] = jnp.ones((64, 256), BF16)

    for chunk in range(4):
        far = far_a_ref[chunk] if chunk < 2 else far_b_ref[chunk - 2]
        pieces = (own_ref[chunk], next_ref[chunk], far, last_ref[chunk])
        for d in range(4):
            put_keys(chunk, d, pieces[d])

    key_lane = lax.broadcasted_iota(jnp.int32, (1, 1024), 1)
    key_d = key_lane // 256
    first_masked = jnp.maximum(zh - jnp.where(zl == 0, 1, 0), 0)

    def row_block(r, _):
        start = pl.multiple_of(r * block, block)
        q = qa[pl.ds(start, block), :]
        row = start + lax.broadcasted_iota(jnp.int32, (block, 1), 0)
        query_pos = z * group - HALO + jnp.where(row >= rows, row - rows, row)

        def step(masked, chunk, state):
            top, acc = state
            s = lax.dot_general(q, ka[chunk], (((1,), (0,)), ((), ())), preferred_element_type=F32)
            if masked:
                turn = zl + key_d
                key_z = 4 * chunk + jnp.where(turn >= 4, turn - 4, turn)
                key_pos = key_z * group + y * 256 + (key_lane - 256 * key_d)
                s = jnp.where(query_pos >= key_pos, s, MASKED)
            new_top = jnp.maximum(top, jnp.max(s, axis=1, keepdims=True))
            p = jnp.exp(s - new_top).astype(BF16)
            more = lax.dot_general(p, va[chunk], (((1,), (1,)), ((), ())), preferred_element_type=F32)
            return new_top, acc * jnp.exp(top - new_top) + more

        state = (jnp.full((block, 1), MASKED, F32), jnp.zeros((block, 128), F32))
        state = lax.fori_loop(0, first_masked, functools.partial(step, False), state)
        top, acc = lax.fori_loop(first_masked, zh + 1, functools.partial(step, True), state)
        total = acc[:, 64:65]
        gate = jnp.where(row >= rows, gate_ref[1], gate_ref[0])
        norm_out[pl.ds(start, block), :] = acc / total
        lse_rows[pl.ds(start, block), :] = jnp.broadcast_to(top + jnp.log(total) - gate, (block, 128))
        return 0

    lax.fori_loop(0, 2 * rows // block, row_block, 0)
    tail = lse_rows.shape[0] - 2 * rows
    lse_rows[pl.ds(2 * rows, tail), :] = jnp.zeros((tail, 128), F32)
    lse_dense[...] = jnp.zeros(lse_dense.shape, F32)
    diagonal = lax.broadcasted_iota(jnp.int32, (128, 128), 0) == lax.broadcasted_iota(jnp.int32, (128, 128), 1)
    pair_rows = HALO + 512
    for pair in range(2):
        a = norm_out[pl.ds(512 * pair, pair_rows), :]
        b = norm_out[pl.ds(rows + 512 * pair, pair_rows), :]
        joined = jnp.where(lane < 64, a, pltpu.roll(b, 64, 1)).astype(BF16)
        for head in range(2):
            for t in range(5):
                tile = lse_rows[pl.ds(head * rows + 512 * pair + 128 * t, 128), :]
                lse_dense[pl.ds(5 * head + t, 1), :] = jnp.sum(jnp.where(diagonal, tile, 0.0), axis=0, keepdims=True)
        parts = split3(lse_dense[...])
        for i in range(2):
            out_ref[2 * pair + i, 0:pair_rows, :] = joined
            for k in range(3):
                out_ref[2 * pair + i, pair_rows + 16 * k:pair_rows + 16 * (k + 1), :] = parts[k]


def attend(at, gate, queries, own, nxt, far_a, far_b, last):
    rows = HALO + 1024
    pair_rows = HALO + 512
    smem = pl.BlockSpec(memory_space=pltpu.SMEM)
    vmem = pl.BlockSpec(memory_space=pltpu.VMEM)
    return pl.pallas_call(
        functools.partial(attend_kernel, rows=rows, block=416),
        out_shape=jax.ShapeDtypeStruct((4, pair_rows + 48, 128), BF16),
        in_specs=[smem, smem] + [vmem] * 6,
        out_specs=vmem,
        scratch_shapes=[
            pltpu.VMEM((2 * rows, 128), BF16),
            pltpu.VMEM((4, 128, 1024), BF16),
            pltpu.VMEM((4, 128, 1024), BF16),
            pltpu.VMEM((2 * rows, 128), F32),
            pltpu.VMEM((2 * rows + 112, 128), F32),
            pltpu.VMEM((16, 128), F32),
        ],
        compiler_params=pltpu.CompilerParams(vmem_limit_bytes=24 * 2**20),
        cost_estimate=pl.CostEstimate(flops=8 * 10**9, bytes_accessed=4 * 2**20, transcendentals=8 * 10**6),
        name="attend",
    )(at, gate, queries, own, nxt, far_a, far_b, last)


def merge_kernel(in_ref, out_ref):
    pair_rows = HALO + 512
    logs = []
    for i in range(4):
        parts = [in_ref[i, pair_rows + 16 * k:pair_rows + 16 * (k + 1), :].astype(F32) for k in range(3)]
        logs.append(parts[0] + parts[1] + parts[2])
    top = jnp.maximum(jnp.maximum(logs[0], logs[1]), jnp.maximum(logs[2], logs[3]))
    weights = [jnp.exp(v - top) for v in logs]
    total = weights[0] + weights[1] + weights[2] + weights[3]
    shares = [w / total for w in weights]
    lane = lax.broadcasted_iota(jnp.int32, (1, 128), 1)
    for t in range(5):
        size = 128 if t < 4 else pair_rows - 512
        diagonal = lax.broadcasted_iota(jnp.int32, (size, 128), 0) == lax.broadcasted_iota(jnp.int32, (size, 128), 1)
        acc = jnp.zeros((size, 128), F32)
        for i in range(4):
            cols = [
                jnp.sum(jnp.where(diagonal, shares[i][5 * head + t:5 * head + t + 1, :], 0.0), axis=1, keepdims=True)
                for head in range(2)
            ]
            share = jnp.where(lane < 64, cols[0], cols[1])
            acc = acc + share * in_ref[i, 128 * t:128 * t + size, :].astype(F32)
        out_ref[128 * t:128 * t + size, :] = acc.astype(BF16)


def merge(pieces):
    vmem = pl.BlockSpec(memory_space=pltpu.VMEM)
    return pl.pallas_call(
        merge_kernel,
        out_shape=jax.ShapeDtypeStruct((HALO + 512, 128), BF16),
        in_specs=[vmem],
        out_specs=vmem,
        compiler_params=pltpu.CompilerParams(vmem_limit_bytes=8 * 2**20),
        cost_estimate=pl.CostEstimate(flops=10**8, bytes_accessed=2**20, transcendentals=10**4),
        name="merge",
    )(pieces)


def feed_kernel(at_ref, attn_own, attn_other, out_own, out_other, resid_own, resid_other, gain_ref, conv_ref, w_ref,
                keep_ref, send_ref, mid_out_ref, af, mid, normed, wg, wu, wd, sems):
    copies = []
    for k, dst in enumerate((wg, wu, wd)):
        copy = pltpu.make_async_copy(w_ref.at[:, :, k], dst, sems.at[k])
        copy.start()
        copies.append(copy)
    is_first, half, core = at_ref[3], at_ref[4], at_ref[6]
    block = at_ref[5]
    rows = HALO + 512
    at_x = block // 2
    sides = ((core, attn_own, out_own, resid_own, keep_ref), (1 - core, attn_other, out_other, resid_other, send_ref))
    for c, attn, _, _, _ in sides:
        for x in range(4):
            af[:, pl.ds(pl.multiple_of(128 * (2 * x + c), 128), 128)] = attn[x]
    a = af[...]
    square = jnp.zeros((rows, 1), F32)
    for c, _, out, resid, _ in sides:
        for i, back in enumerate((0, 1, 3, 2)):
            x = jnp.where(at_x >= back, at_x - back, at_x - back + 4)
            branch = jnp.dot(a, out[i], preferred_element_type=F32)
            m = (branch + resid[x].astype(F32)).astype(BF16)
            mid[:, pl.ds(pl.multiple_of(256 * (2 * x + c), 256), 256)] = m
            m = m.astype(F32)
            square = square + jnp.sum(m * m, axis=1, keepdims=True)
    inverse = lax.rsqrt(square * (1.0 / 2048) + NORM_EPS)
    for j in range(8):
        cols = slice(256 * j, 256 * (j + 1))
        normed[:, cols] = (mid[:, cols].astype(F32) * inverse * gain_ref[:, cols]).astype(BF16)
    mid_out_ref[...] = mid[pl.ds(pl.multiple_of(HALO + 256 * half, 16), 256), pl.ds(pl.multiple_of(256 * block, 256), 256)]
    n = normed[...]
    copies[0].wait()
    copies[1].wait()
    row = lax.broadcasted_iota(jnp.int32, (rows, 1), 0)
    keep = jnp.logical_not((row < HALO) & (is_first == 1))

    def mixed(weight, index):
        pre = jnp.dot(n, weight[...].reshape(2048, 352), preferred_element_type=F32).astype(BF16).astype(F32)
        pre = jnp.where(keep, pre, 0.0)
        total = jnp.zeros((512, 352), F32)
        for k in range(3):
            total = total + conv_ref[2 * k + index:2 * k + index + 1, :] * pre[HALO - 2 + k:HALO - 2 + k + 512]
        return total

    gate = mixed(wg, 0)
    up = mixed(wu, 1)
    hidden = (gate / (1.0 + jnp.exp(-gate)) * up).astype(BF16)
    copies[2].wait()
    for c, _, _, _, part_ref in sides:
        for x in range(4):
            down = wd[pl.ds(2 * (2 * x + c), 2)].reshape(256, 352)
            part = lax.dot_general(hidden, down, (((1,), (1,)), ((), ())), preferred_element_type=F32).astype(BF16)
            for p in range(2):
                part_ref[p, x] = part[256 * p:256 * (p + 1)]


def feed(at, attn, other_attn, out, other_out, resid, other_resid, gain, conv, weights):
    smem = pl.BlockSpec(memory_space=pltpu.SMEM)
    vmem = pl.BlockSpec(memory_space=pltpu.VMEM)
    rows = HALO + 512
    half = jax.ShapeDtypeStruct((2, 4, 256, 256), BF16)
    return pl.pallas_call(
        feed_kernel,
        out_shape=(half, half, jax.ShapeDtypeStruct((256, 256), BF16)),
        in_specs=[smem] + [vmem] * 8 + [pl.BlockSpec(memory_space=pltpu.HBM)],
        out_specs=(vmem, vmem, vmem),
        scratch_shapes=[
            pltpu.VMEM((rows, 1024), BF16),
            pltpu.VMEM((rows, 2048), BF16),
            pltpu.VMEM((rows, 2048), BF16),
            pltpu.VMEM((16, 4, 32, 352), BF16),
            pltpu.VMEM((16, 4, 32, 352), BF16),
            pltpu.VMEM((16, 4, 32, 352), BF16),
            pltpu.SemaphoreType.DMA((3,)),
        ],
        compiler_params=pltpu.CompilerParams(vmem_limit_bytes=40 * 2**20),
        cost_estimate=pl.CostEstimate(flops=5 * 10**9, bytes_accessed=2**24, transcendentals=2 * 10**5),
        name="feed",
    )(at, attn, other_attn, out, other_out, resid, other_resid, gain, conv, weights)


def keys_kernel(kv_ref, gate_ref, out_ref):
    turned = kv_ref[0].astype(F32).T.astype(BF16)
    row = lax.broadcasted_iota(jnp.int32, (16, 256), 0)
    value = jnp.where(row < 3, gate_ref[0:1, :], gate_ref[1:2, :])
    which = jnp.where(row < 3, row, row - 3)
    high, middle, low = split3(value)
    pick = jnp.where(which == 0, high.astype(F32), jnp.where(which == 1, middle.astype(F32), low.astype(F32)))
    gates = jnp.where(row < 6, pick, 0.0).astype(BF16)
    for i in range(4):
        out_ref[i, 0:64, :] = turned[0:64]
        out_ref[i, 64:80, :] = gates
        out_ref[i, 80:144, :] = turned[64:128]


def halves_kernel(gate_ref, up_ref, down_ref, out_ref):
    for k, ref in enumerate((gate_ref, up_ref, down_ref)):
        value = ref[...].astype(F32)
        for p in range(2):
            piece = value[:, 352 * p:352 * (p + 1)].astype(BF16)
            for i in range(2):
                out_ref[2 * i + p, k] = piece


def small_call(kernel, shape, *operands):
    vmem = pl.BlockSpec(memory_space=pltpu.VMEM)
    return pl.pallas_call(
        kernel,
        out_shape=jax.ShapeDtypeStruct(shape, BF16),
        in_specs=[vmem] * len(operands),
        out_specs=vmem,
        compiler_params=pltpu.CompilerParams(vmem_limit_bytes=8 * 2**20),
        cost_estimate=pl.CostEstimate(flops=10**7, bytes_accessed=2**20, transcendentals=0),
    )(*operands)


def layer(resid, queries, keys_values, cum_gate, out_weight, norm_gain, gate_weight, up_weight, conv_kernel, down_weight):
    zh, zl = lax.axis_index("zh"), lax.axis_index("zl")
    y, half = lax.axis_index(Y), lax.axis_index("yl")
    is_first = (lax.axis_index(SP) < 2).astype(jnp.int32)
    at = jnp.stack([zh, zl, y, is_first, half, lax.axis_index(TP), lax.axis_index("c")]).astype(jnp.int32)

    own = exchanged(small_call(keys_kernel, (4, 144, 256), keys_values, cum_gate), "zh")
    rows_y = exchanged(small_call(halves_kernel, (4, 3, 32, 352), gate_weight, up_weight, down_weight.T), Y)
    weights = lax.all_gather(rows_y, Z, axis=0, tiled=False)
    tail = jnp.concatenate([queries[-HALO:], resid[-HALO:]], axis=1)
    before = shifted(tail, SP, 1)
    out = jnp.stack([out_weight] + [shifted(out_weight, "x", by) for by in (1, 3, 2)])
    other_out = shifted(out, "c", 1)
    group_q = spread(jnp.concatenate([before[:, :128], queries], axis=0), Y)
    last = shifted(own, Z, 1)
    nxt = shifted(own, Z, -1)
    far_a = shifted(own[:2], Z, -2)
    far_b = shifted(own[2:], Z, 2)
    mine = jnp.concatenate([before[:, 128:], resid], axis=0)
    theirs = shifted(mine, "yl", 1)
    pair = jnp.where(
        half == 0,
        jnp.concatenate([mine, theirs[HALO:]], axis=0),
        jnp.concatenate([theirs, mine[HALO:]], axis=0),
    )
    pair = spread(pair, "x")
    other_pair = shifted(pair, "c", 1)

    partial = attend(at, cum_gate[:, 0], group_q, own, nxt, far_a, far_b, last)
    partial = exchanged(partial, Y)
    attn = merge(partial)
    attn = lax.all_gather(attn, "x", axis=0, tiled=False)
    other_attn = shifted(attn, "c", 1)
    conv = lax.dynamic_slice_in_dim(conv_kernel.reshape(6, 704), half * 352, 352, 1)
    keep, send, middle = feed(
        at, attn, other_attn, out, other_out, pair, other_pair, norm_gain.reshape(1, 2048), conv, weights
    )
    got = shifted(send, "c", 1)
    chip = (keep.astype(F32) + got.astype(F32)).astype(BF16).reshape(8, 256, 256)
    pieces = exchanged(chip, ("yl", "x"))
    total = jnp.sum(pieces.astype(F32), axis=0)
    return (middle.astype(F32) + total).astype(BF16)


def solution(mesh):
    finer = Mesh(mesh.devices.reshape(4, 4, 2, 2, 4, 2), SP + TP)
    return jax.shard_map(
        layer,
        mesh=finer,
        in_specs=(
            P(SP, TP),
            P(SP, TP),
            P(TP, SP, None),
            P(TP, SP),
            P(None, TP),
            P(),
            P(SP, TP),
            P(SP, TP),
            P(None, None, TP),
            P(TP, SP),
        ),
        out_specs=P(SP, TP),
        check_vma=False,
    )
```

```python
import functools

import jax
import jax.numpy as jnp
from jax import lax
from jax.experimental import pallas as pl
from jax.experimental.pallas import tpu as pltpu
from jax.sharding import Mesh
from jax.sharding import PartitionSpec as P


Z = ("zh", "zl")
Y = ("yh", "yl")
SP = Z + Y
TP = ("x", "c")
NORM_EPS = 1e-06
HALO = 16
MASKED = -1e30
F32 = jnp.float32
BF16 = jnp.bfloat16


def shifted(value, axis, by):
    size = lax.axis_size(axis)
    return lax.ppermute(value, axis, [(i, (i + by) % size) for i in range(size)])


def exchanged(value, axis):
    return lax.all_to_all(value, axis, 0, 0, tiled=True)


def spread(value, axis):
    size = lax.axis_size(axis)
    return exchanged(jnp.broadcast_to(value[None], (size, *value.shape)), axis)


def split3(value):
    high = value.astype(BF16)
    rest = value - high.astype(F32)
    middle = rest.astype(BF16)
    low = (rest - middle.astype(F32)).astype(BF16)
    return high, middle, low


def attend_kernel(at_ref, gate_ref, q_ref, own_ref, next_ref, far_a_ref, far_b_ref, last_ref,
                  out_ref, qa, ka, va, norm_out, lse_rows, lse_dense, *, rows, block):
    zh, zl, y = at_ref[0], at_ref[1], at_ref[2]
    z = 4 * zh + zl
    lane = lax.broadcasted_iota(jnp.int32, (1, 128), 1)
    group = rows - HALO

    def put_queries(start, piece):
        x = piece.astype(F32) * 0.125
        for head in range(2):
            part = x if head == 0 else pltpu.roll(x, 64, 1)
            first = 64 + 3 * head
            ones = jnp.where((lane >= first) & (lane < first + 3), 1.0, 0.0)
            both = jnp.where(lane < 64, part, ones)
            qa[pl.ds(head * rows + start, piece.shape[0]), :] = both.astype(BF16)

    put_queries(0, q_ref[0, 0:HALO, :])
    for i in range(4):
        put_queries(HALO + 256 * i, q_ref[i, HALO:HALO + 256, :])

    part_row = lax.broadcasted_iota(jnp.int32, (16, 256), 0)

    def put_keys(chunk, d, piece):
        cols = pl.ds(256 * d, 256)
        ka[chunk, 0:64, cols] = piece[0:64, :]
        g = piece[64:80, :].astype(F32)
        bias = []
        for head in range(2):
            total = g[3 * head:3 * head + 1, :] + g[3 * head + 1:3 * head + 2, :]
            bias.append(gate_ref[head] - (total + g[3 * head + 2:3 * head + 3, :]))
        b = jnp.where(part_row < 3, bias[0], bias[1])
        which = jnp.where(part_row < 3, part_row, part_row - 3)
        high, middle, low = split3(b)
        pick = jnp.where(which == 0, high.astype(F32), jnp.where(which == 1, middle.astype(F32), low.astype(F32)))
        ka[chunk, 64:80, cols] = jnp.where(part_row < 6, pick, 0.0).astype(BF16)
        ka[chunk, 80:128, cols] = jnp.zeros((48, 256), BF16)
        va[chunk, 0:64, cols] = piece[80:144, :]
        va[chunk, 64:128, cols] = jnp.ones((64, 256), BF16)

    for chunk in range(4):
        far = far_a_ref[chunk] if chunk < 2 else far_b_ref[chunk - 2]
        pieces = (own_ref[chunk], next_ref[chunk], far, last_ref[chunk])
        for d in range(4):
            put_keys(chunk, d, pieces[d])

    key_lane = lax.broadcasted_iota(jnp.int32, (1, 1024), 1)
    key_d = key_lane // 256
    first_masked = jnp.maximum(zh - jnp.where(zl == 0, 1, 0), 0)

    def row_block(r, _):
        start = pl.multiple_of(r * block, block)
        q = qa[pl.ds(start, block), :]
        row = start + lax.broadcasted_iota(jnp.int32, (block, 1), 0)
        query_pos = z * group - HALO + jnp.where(row >= rows, row - rows, row)

        def step(masked, chunk, state):
            top, acc = state
            s = lax.dot_general(q, ka[chunk], (((1,), (0,)), ((), ())), preferred_element_type=F32)
            if masked:
                turn = zl + key_d
                key_z = 4 * chunk + jnp.where(turn >= 4, turn - 4, turn)
                key_pos = key_z * group + y * 256 + (key_lane - 256 * key_d)
                s = jnp.where(query_pos >= key_pos, s, MASKED)
            new_top = jnp.maximum(top, jnp.max(s, axis=1, keepdims=True))
            p = jnp.exp(s - new_top).astype(BF16)
            more = lax.dot_general(p, va[chunk], (((1,), (1,)), ((), ())), preferred_element_type=F32)
            return new_top, acc * jnp.exp(top - new_top) + more

        state = (jnp.full((block, 1), MASKED, F32), jnp.zeros((block, 128), F32))
        state = lax.fori_loop(0, first_masked, functools.partial(step, False), state)
        top, acc = lax.fori_loop(first_masked, zh + 1, functools.partial(step, True), state)
        total = acc[:, 64:65]
        gate = jnp.where(row >= rows, gate_ref[1], gate_ref[0])
        norm_out[pl.ds(start, block), :] = acc / total
        lse_rows[pl.ds(start, block), :] = jnp.broadcast_to(top + jnp.log(total) - gate, (block, 128))
        return 0

    lax.fori_loop(0, 2 * rows // block, row_block, 0)
    tail = lse_rows.shape[0] - 2 * rows
    lse_rows[pl.ds(2 * rows, tail), :] = jnp.zeros((tail, 128), F32)
    lse_dense[...] = jnp.zeros(lse_dense.shape, F32)
    diagonal = lax.broadcasted_iota(jnp.int32, (128, 128), 0) == lax.broadcasted_iota(jnp.int32, (128, 128), 1)
    pair_rows = HALO + 512
    for pair in range(2):
        a = norm_out[pl.ds(512 * pair, pair_rows), :]
        b = norm_out[pl.ds(rows + 512 * pair, pair_rows), :]
        joined = jnp.where(lane < 64, a, pltpu.roll(b, 64, 1)).astype(BF16)
        for head in range(2):
            for t in range(5):
                tile = lse_rows[pl.ds(head * rows + 512 * pair + 128 * t, 128), :]
                lse_dense[pl.ds(5 * head + t, 1), :] = jnp.sum(jnp.where(diagonal, tile, 0.0), axis=0, keepdims=True)
        parts = split3(lse_dense[...])
        for i in range(2):
            out_ref[2 * pair + i, 0:pair_rows, :] = joined
            for k in range(3):
                out_ref[2 * pair + i, pair_rows + 16 * k:pair_rows + 16 * (k + 1), :] = parts[k]


def attend(at, gate, queries, own, nxt, far_a, far_b, last):
    rows = HALO + 1024
    pair_rows = HALO + 512
    smem = pl.BlockSpec(memory_space=pltpu.SMEM)
    vmem = pl.BlockSpec(memory_space=pltpu.VMEM)
    return pl.pallas_call(
        functools.partial(attend_kernel, rows=rows, block=416),
        out_shape=jax.ShapeDtypeStruct((4, pair_rows + 48, 128), BF16),
        in_specs=[smem, smem] + [vmem] * 6,
        out_specs=vmem,
        scratch_shapes=[
            pltpu.VMEM((2 * rows, 128), BF16),
            pltpu.VMEM((4, 128, 1024), BF16),
            pltpu.VMEM((4, 128, 1024), BF16),
            pltpu.VMEM((2 * rows, 128), F32),
            pltpu.VMEM((2 * rows + 112, 128), F32),
            pltpu.VMEM((16, 128), F32),
        ],
        compiler_params=pltpu.CompilerParams(vmem_limit_bytes=24 * 2**20),
        cost_estimate=pl.CostEstimate(flops=8 * 10**9, bytes_accessed=4 * 2**20, transcendentals=8 * 10**6),
        name="attend",
    )(at, gate, queries, own, nxt, far_a, far_b, last)


def merge_kernel(in_ref, out_ref):
    pair_rows = HALO + 512
    logs = []
    for i in range(4):
        parts = [in_ref[i, pair_rows + 16 * k:pair_rows + 16 * (k + 1), :].astype(F32) for k in range(3)]
        logs.append(parts[0] + parts[1] + parts[2])
    top = jnp.maximum(jnp.maximum(logs[0], logs[1]), jnp.maximum(logs[2], logs[3]))
    weights = [jnp.exp(v - top) for v in logs]
    total = weights[0] + weights[1] + weights[2] + weights[3]
    shares = [w / total for w in weights]
    lane = lax.broadcasted_iota(jnp.int32, (1, 128), 1)
    for t in range(5):
        size = 128 if t < 4 else pair_rows - 512
        diagonal = lax.broadcasted_iota(jnp.int32, (size, 128), 0) == lax.broadcasted_iota(jnp.int32, (size, 128), 1)
        acc = jnp.zeros((size, 128), F32)
        for i in range(4):
            cols = [
                jnp.sum(jnp.where(diagonal, shares[i][5 * head + t:5 * head + t + 1, :], 0.0), axis=1, keepdims=True)
                for head in range(2)
            ]
            share = jnp.where(lane < 64, cols[0], cols[1])
            acc = acc + share * in_ref[i, 128 * t:128 * t + size, :].astype(F32)
        out_ref[128 * t:128 * t + size, :] = acc.astype(BF16)


def merge(pieces):
    vmem = pl.BlockSpec(memory_space=pltpu.VMEM)
    return pl.pallas_call(
        merge_kernel,
        out_shape=jax.ShapeDtypeStruct((HALO + 512, 128), BF16),
        in_specs=[vmem],
        out_specs=vmem,
        compiler_params=pltpu.CompilerParams(vmem_limit_bytes=8 * 2**20),
        cost_estimate=pl.CostEstimate(flops=10**8, bytes_accessed=2**20, transcendentals=10**4),
        name="merge",
    )(pieces)


def feed_kernel(at_ref, attn_own, attn_other, wide_own, wide_other, gain_ref, conv_ref, w_ref,
                keep_ref, send_ref, mid_out_ref, af, mid, normed, wg, wu, wd, sems):
    copies = []
    for k, dst in enumerate((wg, wu, wd)):
        copy = pltpu.make_async_copy(w_ref.at[:, :, k], dst, sems.at[k])
        copy.start()
        copies.append(copy)
    is_first, half, core = at_ref[3], at_ref[4], at_ref[6]
    block = at_ref[5]
    rows = HALO + 512
    at_x = block // 2
    sides = ((core, attn_own, wide_own, keep_ref), (1 - core, attn_other, wide_other, send_ref))
    for c, attn, _, _ in sides:
        for x in range(4):
            af[:, pl.ds(pl.multiple_of(128 * (2 * x + c), 128), 128)] = attn[x]
    a = af[...]
    square = jnp.zeros((rows, 1), F32)
    for c, _, wide, _ in sides:
        for i, back in enumerate((0, 1, 3, 2)):
            x = jnp.where(at_x >= back, at_x - back, at_x - back + 4)
            branch = jnp.dot(a, wide[i, 0:1024, :], preferred_element_type=F32)
            m = (branch + wide[i, 1024:1024 + rows, :].astype(F32)).astype(BF16)
            mid[:, pl.ds(pl.multiple_of(256 * (2 * x + c), 256), 256)] = m
            m = m.astype(F32)
            square = square + jnp.sum(m * m, axis=1, keepdims=True)
    inverse = lax.rsqrt(square * (1.0 / 2048) + NORM_EPS)
    for j in range(8):
        cols = slice(256 * j, 256 * (j + 1))
        normed[:, cols] = (mid[:, cols].astype(F32) * inverse * gain_ref[:, cols]).astype(BF16)
    mid_out_ref[...] = mid[pl.ds(pl.multiple_of(HALO + 256 * half, 16), 256), pl.ds(pl.multiple_of(256 * block, 256), 256)]
    n = normed[...]
    copies[0].wait()
    copies[1].wait()
    row = lax.broadcasted_iota(jnp.int32, (rows, 1), 0)
    keep = jnp.logical_not((row < HALO) & (is_first == 1))

    def mixed(weight, index):
        pre = jnp.dot(n, weight[...].reshape(2048, 352), preferred_element_type=F32).astype(BF16).astype(F32)
        pre = jnp.where(keep, pre, 0.0)
        total = jnp.zeros((512, 352), F32)
        for k in range(3):
            total = total + conv_ref[2 * k + index:2 * k + index + 1, :] * pre[HALO - 2 + k:HALO - 2 + k + 512]
        return total

    gate = mixed(wg, 0)
    up = mixed(wu, 1)
    hidden = (gate / (1.0 + jnp.exp(-gate)) * up).astype(BF16)
    copies[2].wait()
    for c, _, _, part_ref in sides:
        for x in range(4):
            down = wd[pl.ds(2 * (2 * x + c), 2)].reshape(256, 352)
            part = lax.dot_general(hidden, down, (((1,), (1,)), ((), ())), preferred_element_type=F32).astype(BF16)
            for p in range(2):
                part_ref[p, x] = part[256 * p:256 * (p + 1)]


def feed(at, attn, other_attn, wide, other_wide, gain, conv, weights):
    smem = pl.BlockSpec(memory_space=pltpu.SMEM)
    vmem = pl.BlockSpec(memory_space=pltpu.VMEM)
    rows = HALO + 512
    half = jax.ShapeDtypeStruct((2, 4, 256, 256), BF16)
    return pl.pallas_call(
        feed_kernel,
        out_shape=(half, half, jax.ShapeDtypeStruct((256, 256), BF16)),
        in_specs=[smem] + [vmem] * 6 + [pl.BlockSpec(memory_space=pltpu.HBM)],
        out_specs=(vmem, vmem, vmem),
        scratch_shapes=[
            pltpu.VMEM((rows, 1024), BF16),
            pltpu.VMEM((rows, 2048), BF16),
            pltpu.VMEM((rows, 2048), BF16),
            pltpu.VMEM((16, 4, 32, 352), BF16),
            pltpu.VMEM((16, 4, 32, 352), BF16),
            pltpu.VMEM((16, 4, 32, 352), BF16),
            pltpu.SemaphoreType.DMA((3,)),
        ],
        compiler_params=pltpu.CompilerParams(vmem_limit_bytes=50 * 2**20),
        cost_estimate=pl.CostEstimate(flops=5 * 10**9, bytes_accessed=2**24, transcendentals=2 * 10**5),
        name="feed",
    )(at, attn, other_attn, wide, other_wide, gain, conv, weights)


def prepare_kernel(kv_ref, decay_ref, gate_ref, up_ref, down_ref, q_ref, resid_ref, keys_ref, halves_ref, tail_ref):
    turned = kv_ref[0].astype(F32).T.astype(BF16)
    row = lax.broadcasted_iota(jnp.int32, (16, 256), 0)
    value = jnp.where(row < 3, decay_ref[0:1, :], decay_ref[1:2, :])
    which = jnp.where(row < 3, row, row - 3)
    high, middle, low = split3(value)
    pick = jnp.where(which == 0, high.astype(F32), jnp.where(which == 1, middle.astype(F32), low.astype(F32)))
    gates = jnp.where(row < 6, pick, 0.0).astype(BF16)
    for i in range(4):
        keys_ref[i, 0:64, :] = turned[0:64]
        keys_ref[i, 64:80, :] = gates
        keys_ref[i, 80:144, :] = turned[64:128]
    for k, ref in enumerate((gate_ref, up_ref, down_ref)):
        value = ref[...].astype(F32)
        for p in range(2):
            piece = value[:, 352 * p:352 * (p + 1)].astype(BF16)
            for i in range(2):
                halves_ref[2 * i + p, k] = piece
    tail_ref[:, 0:128] = q_ref[256 - HALO:256, :]
    tail_ref[:, 128:384] = resid_ref[256 - HALO:256, :]


def prepare(*operands):
    vmem = pl.BlockSpec(memory_space=pltpu.VMEM)
    return pl.pallas_call(
        prepare_kernel,
        out_shape=(
            jax.ShapeDtypeStruct((4, 144, 256), BF16),
            jax.ShapeDtypeStruct((4, 3, 32, 352), BF16),
            jax.ShapeDtypeStruct((HALO, 384), BF16),
        ),
        in_specs=[vmem] * len(operands),
        out_specs=(vmem, vmem, vmem),
        cost_estimate=pl.CostEstimate(flops=10**7, bytes_accessed=2**20, transcendentals=0),
        name="prepare",
    )(*operands)


def layer(resid, queries, keys_values, cum_gate, out_weight, norm_gain, gate_weight, up_weight, conv_kernel, down_weight):
    zh, zl = lax.axis_index("zh"), lax.axis_index("zl")
    y, half = lax.axis_index(Y), lax.axis_index("yl")
    is_first = (lax.axis_index(SP) < 2).astype(jnp.int32)
    at = jnp.stack([zh, zl, y, is_first, half, lax.axis_index(TP), lax.axis_index("c")]).astype(jnp.int32)

    keys, halves, tail = prepare(
        keys_values, cum_gate, gate_weight, up_weight, down_weight.T, queries, resid
    )
    before = shifted(tail, SP, 1)
    rows_y = exchanged(halves, Y)
    weights = lax.all_gather(rows_y, Z, axis=0, tiled=False)
    mine = jnp.concatenate([before[:, 128:], resid], axis=0)
    theirs = shifted(mine, "yl", 1)
    own = exchanged(keys, "zh")
    low = jnp.concatenate([out_weight, mine, theirs[HALO:]], axis=0)
    high = jnp.concatenate([out_weight, theirs, mine[HALO:]], axis=0)
    wide = jnp.where(half == 0, low, high)
    wides = [wide] + [shifted(wide, "x", by) for by in (1, 3, 2)]
    last = shifted(own, Z, 1)
    nxt = shifted(own, Z, -1)
    far_a = shifted(own[:2], Z, -2)
    far_b = shifted(own[2:], Z, 2)
    group_q = spread(jnp.concatenate([before[:, :128], queries], axis=0), Y)

    partial = attend(at, cum_gate[:, 0], group_q, own, nxt, far_a, far_b, last)
    partial = exchanged(partial, Y)
    wide = jnp.stack(wides)
    other_wide = shifted(wide, "c", 1)
    attn = merge(partial)
    attn = lax.all_gather(attn, "x", axis=0, tiled=False)
    other_attn = shifted(attn, "c", 1)
    conv = lax.dynamic_slice_in_dim(conv_kernel.reshape(6, 704), half * 352, 352, 1)
    keep, send, middle = feed(
        at, attn, other_attn, wide, other_wide, norm_gain.reshape(1, 2048), conv, weights
    )
    got = shifted(send, "c", 1)
    chip = (keep.astype(F32) + got.astype(F32)).astype(BF16).reshape(8, 256, 256)
    pieces = exchanged(chip, ("yl", "x"))
    total = jnp.sum(pieces.astype(F32), axis=0)
    return (middle.astype(F32) + total).astype(BF16)


def solution(mesh):
    finer = Mesh(mesh.devices.reshape(4, 4, 2, 2, 4, 2), SP + TP)
    return jax.shard_map(
        layer,
        mesh=finer,
        in_specs=(
            P(SP, TP),
            P(SP, TP),
            P(TP, SP, None),
            P(TP, SP),
            P(None, TP),
            P(),
            P(SP, TP),
            P(SP, TP),
            P(None, None, TP),
            P(TP, SP),
        ),
        out_specs=P(SP, TP),
        check_vma=False,
    )
```

```python
import functools

import jax
import jax.numpy as jnp
from jax import lax
from jax.experimental import pallas as pl
from jax.experimental.pallas import tpu as pltpu
from jax.sharding import Mesh
from jax.sharding import PartitionSpec as P


Z = ("zh", "zl")
Y = ("yh", "yl")
SP = Z + Y
TP = ("x", "c")
NORM_EPS = 1e-06
HALO = 16
MASKED = -1e30
F32 = jnp.float32
BF16 = jnp.bfloat16


def shifted(value, axis, by):
    size = lax.axis_size(axis)
    return lax.ppermute(value, axis, [(i, (i + by) % size) for i in range(size)])


def exchanged(value, axis):
    return lax.all_to_all(value, axis, 0, 0, tiled=True)


def spread(value, axis):
    size = lax.axis_size(axis)
    return exchanged(jnp.broadcast_to(value[None], (size, *value.shape)), axis)


def split3(value):
    high = value.astype(BF16)
    rest = value - high.astype(F32)
    middle = rest.astype(BF16)
    low = (rest - middle.astype(F32)).astype(BF16)
    return high, middle, low


def put_keys(ka, va, chunk, d, piece, gate_ref):
    cols = pl.ds(256 * d, 256)
    row = lax.broadcasted_iota(jnp.int32, (8, 256), 0)
    ka[chunk, 0:64, cols] = piece[0:64, :]
    g = piece[64:72, :].astype(F32)
    bias = []
    for head in range(2):
        total = g[3 * head:3 * head + 1, :] + g[3 * head + 1:3 * head + 2, :]
        bias.append(gate_ref[head] - (total + g[3 * head + 2:3 * head + 3, :]))
    b = jnp.where(row < 3, bias[0], bias[1])
    which = jnp.where(row < 3, row, row - 3)
    high, middle, low = split3(b)
    pick = jnp.where(which == 0, high.astype(F32), jnp.where(which == 1, middle.astype(F32), low.astype(F32)))
    ka[chunk, 64:72, cols] = jnp.where(row < 6, pick, 0.0).astype(BF16)
    ka[chunk, 72:128, cols] = jnp.zeros((56, 256), BF16)
    va[chunk, 0:64, cols] = piece[72:136, :]
    va[chunk, 64:128, cols] = jnp.ones((64, 256), BF16)


def fold_keys(queries, keys, values, state, query_pos, key_pos):
    scores = []
    for i, q in enumerate(queries):
        s = lax.dot_general(q, keys, (((1,), (0,)), ((), ())), preferred_element_type=F32)
        if key_pos is not None:
            s = jnp.where(query_pos[i] >= key_pos, s, MASKED)
        scores.append(s)
    new_state = []
    for s, (top, acc) in zip(scores, state):
        new_top = jnp.maximum(top, jnp.max(s, axis=1, keepdims=True))
        p = jnp.exp(s - new_top).astype(BF16)
        more = lax.dot_general(p, values, (((1,), (1,)), ((), ())), preferred_element_type=F32)
        new_state.append((new_top, acc * jnp.exp(top - new_top) + more))
    return tuple(new_state)


def row_blocks(z):
    rows, part = HALO + 1024, 416
    blocks = []
    for start in range(0, 2 * rows, part):
        row = start + lax.broadcasted_iota(jnp.int32, (part, 1), 0)
        blocks.append((start, row >= rows, z * 1024 - HALO + jnp.where(row >= rows, row - rows, row)))
    return part, blocks


def attend_own_kernel(at_ref, gate_ref, q_ref, own_ref, qa, state_ref, ka, va):
    zh, zl, y = at_ref[0], at_ref[1], at_ref[2]
    z = 4 * zh + zl
    rows = HALO + 1024
    lane = lax.broadcasted_iota(jnp.int32, (1, 128), 1)

    def put_queries(start, piece):
        x = piece.astype(F32) * 0.125
        for head in range(2):
            side = x if head == 0 else pltpu.roll(x, 64, 1)
            first = 64 + 3 * head
            ones = jnp.where((lane >= first) & (lane < first + 3), 1.0, 0.0)
            both = jnp.where(lane < 64, side, ones)
            qa[head * rows + start:head * rows + start + piece.shape[0], :] = both.astype(BF16)

    put_queries(0, q_ref[0, 0:HALO, :])
    for i in range(4):
        put_queries(HALO + 256 * i, q_ref[i, HALO:HALO + 256, :])
    for chunk in range(4):
        put_keys(ka, va, 0, chunk, own_ref[chunk], gate_ref)
    key_lane = lax.broadcasted_iota(jnp.int32, (1, 1024), 1)
    key_chunk = key_lane // 256
    key_pos = (4 * key_chunk + zl) * 1024 + y * 256 + (key_lane - 256 * key_chunk)
    part, blocks = row_blocks(z)
    state = tuple((jnp.full((part, 1), MASKED, F32), jnp.zeros((part, 128), F32)) for _ in blocks)
    queries = [qa[start:start + part, :] for start, _, _ in blocks]
    state = fold_keys(queries, ka[0], va[0], state, [pos for _, _, pos in blocks], key_pos)
    for (start, _, _), (top, acc) in zip(blocks, state):
        state_ref[start:start + part, :] = jnp.where(lane < 96, acc, top)


def attend_own(at, gate, queries, own):
    rows = HALO + 1024
    smem = pl.BlockSpec(memory_space=pltpu.SMEM)
    vmem = pl.BlockSpec(memory_space=pltpu.VMEM)
    return pl.pallas_call(
        attend_own_kernel,
        out_shape=(jax.ShapeDtypeStruct((2 * rows, 128), BF16), jax.ShapeDtypeStruct((2 * rows, 128), F32)),
        in_specs=[smem, smem, vmem, vmem],
        out_specs=(vmem, vmem),
        scratch_shapes=[pltpu.VMEM((1, 128, 1024), BF16), pltpu.VMEM((1, 128, 1024), BF16)],
        compiler_params=pltpu.CompilerParams(vmem_limit_bytes=30 * 2**20),
        cost_estimate=pl.CostEstimate(flops=2 * 10**9, bytes_accessed=2**20, transcendentals=2 * 10**6),
        name="attend_own",
    )(at, gate, queries, own)


def attend_rest_kernel(at_ref, gate_ref, qa, state_ref, next_ref, far_a_ref, far_b_ref, last_ref,
                       out_ref, ka, va, norm_out, lse_rows, lse_dense):
    zh, zl, y = at_ref[0], at_ref[1], at_ref[2]
    z = 4 * zh + zl
    rows = HALO + 1024
    lane = lax.broadcasted_iota(jnp.int32, (1, 128), 1)
    for chunk in range(4):
        far = far_a_ref[chunk] if chunk < 2 else far_b_ref[chunk - 2]
        for d, piece in enumerate((next_ref[chunk], far, last_ref[chunk])):
            put_keys(ka, va, chunk, d, piece, gate_ref)
    key_lane = lax.broadcasted_iota(jnp.int32, (1, 768), 1)
    key_d = key_lane // 256
    turn = zl + 1 + key_d
    turn = jnp.where(turn >= 4, turn - 4, turn)
    key_rest = turn * 1024 + y * 256 + (key_lane - 256 * key_d)
    first_masked = jnp.maximum(zh - jnp.where(zl == 0, 1, 0), 0)
    part, blocks = row_blocks(z)

    def step(masked, chunk, state):
        queries = [qa[start:start + part, :] for start, _, _ in blocks]
        key_pos = chunk * 4096 + key_rest if masked else None
        return fold_keys(queries, ka[chunk], va[chunk], state, [pos for _, _, pos in blocks], key_pos)

    state = []
    for start, _, _ in blocks:
        piece = state_ref[start:start + part, :]
        state.append((piece[:, 127:128], piece))
    state = lax.fori_loop(0, first_masked, functools.partial(step, False), tuple(state))
    state = lax.fori_loop(first_masked, zh + 1, functools.partial(step, True), state)
    for (start, second, _), (top, acc) in zip(blocks, state):
        total = acc[:, 64:65]
        gate = jnp.where(second, gate_ref[1], gate_ref[0])
        norm_out[start:start + part, :] = acc * (1.0 / total)
        lse_rows[start:start + part, :] = jnp.broadcast_to(top + jnp.log(total) - gate, (part, 128))
    tail = lse_rows.shape[0] - 2 * rows
    lse_rows[pl.ds(2 * rows, tail), :] = jnp.zeros((tail, 128), F32)
    lse_dense[...] = jnp.zeros(lse_dense.shape, F32)
    diagonal = lax.broadcasted_iota(jnp.int32, (128, 128), 0) == lax.broadcasted_iota(jnp.int32, (128, 128), 1)
    pair_rows = HALO + 512
    for pair in range(2):
        a = norm_out[pl.ds(512 * pair, pair_rows), :]
        b = norm_out[pl.ds(rows + 512 * pair, pair_rows), :]
        joined = jnp.where(lane < 64, a, pltpu.roll(b, 64, 1)).astype(BF16)
        for head in range(2):
            for t in range(5):
                tile = lse_rows[pl.ds(head * rows + 512 * pair + 128 * t, 128), :]
                lse_dense[pl.ds(5 * head + t, 1), :] = jnp.sum(jnp.where(diagonal, tile, 0.0), axis=0, keepdims=True)
        parts = split3(lse_dense[...])
        for i in range(2):
            out_ref[2 * pair + i, 0:pair_rows, :] = joined
            for k in range(3):
                out_ref[2 * pair + i, pair_rows + 16 * k:pair_rows + 16 * (k + 1), :] = parts[k]


def attend_rest(at, gate, queries, state, nxt, far_a, far_b, last):
    rows = HALO + 1024
    pair_rows = HALO + 512
    smem = pl.BlockSpec(memory_space=pltpu.SMEM)
    vmem = pl.BlockSpec(memory_space=pltpu.VMEM)
    return pl.pallas_call(
        attend_rest_kernel,
        out_shape=jax.ShapeDtypeStruct((4, pair_rows + 48, 128), BF16),
        in_specs=[smem, smem] + [vmem] * 6,
        out_specs=vmem,
        scratch_shapes=[
            pltpu.VMEM((4, 128, 768), BF16),
            pltpu.VMEM((4, 128, 768), BF16),
            pltpu.VMEM((2 * rows, 128), F32),
            pltpu.VMEM((2 * rows + 112, 128), F32),
            pltpu.VMEM((16, 128), F32),
        ],
        compiler_params=pltpu.CompilerParams(vmem_limit_bytes=36 * 2**20),
        cost_estimate=pl.CostEstimate(flops=6 * 10**9, bytes_accessed=4 * 2**20, transcendentals=6 * 10**6),
        name="attend_rest",
    )(at, gate, queries, state, nxt, far_a, far_b, last)


def merge_kernel(in_ref, out_ref):
    pair_rows = HALO + 512
    logs = []
    for i in range(4):
        parts = [in_ref[i, pair_rows + 16 * k:pair_rows + 16 * (k + 1), :].astype(F32) for k in range(3)]
        logs.append(parts[0] + parts[1] + parts[2])
    top = jnp.maximum(jnp.maximum(logs[0], logs[1]), jnp.maximum(logs[2], logs[3]))
    weights = [jnp.exp(v - top) for v in logs]
    total = weights[0] + weights[1] + weights[2] + weights[3]
    shares = [w / total for w in weights]
    lane = lax.broadcasted_iota(jnp.int32, (1, 128), 1)
    for t in range(5):
        size = 128 if t < 4 else pair_rows - 512
        diagonal = lax.broadcasted_iota(jnp.int32, (size, 128), 0) == lax.broadcasted_iota(jnp.int32, (size, 128), 1)
        acc = jnp.zeros((size, 128), F32)
        for i in range(4):
            cols = [
                jnp.sum(jnp.where(diagonal, shares[i][5 * head + t:5 * head + t + 1, :], 0.0), axis=1, keepdims=True)
                for head in range(2)
            ]
            share = jnp.where(lane < 64, cols[0], cols[1])
            acc = acc + share * in_ref[i, 128 * t:128 * t + size, :].astype(F32)
        out_ref[128 * t:128 * t + size, :] = acc.astype(BF16)


def merge(pieces):
    vmem = pl.BlockSpec(memory_space=pltpu.VMEM)
    return pl.pallas_call(
        merge_kernel,
        out_shape=jax.ShapeDtypeStruct((HALO + 512, 128), BF16),
        in_specs=[vmem],
        out_specs=vmem,
        compiler_params=pltpu.CompilerParams(vmem_limit_bytes=8 * 2**20),
        cost_estimate=pl.CostEstimate(flops=10**8, bytes_accessed=2**20, transcendentals=10**4),
        name="merge",
    )(pieces)


def feed_kernel(at_ref, attn_own, attn_other, wide_own, wide_other, gain_ref, conv_ref, w_ref,
                keep_ref, send_ref, mid_out_ref, af, mid, scaled, wide_in, wg, wu, wd, sems):
    fetches = []
    for side, wide in enumerate((wide_own, wide_other)):
        for i in range(4):
            fetch = pltpu.make_async_copy(wide.at[i], wide_in.at[side, i], sems.at[3 + 4 * side + i])
            fetch.start()
            fetches.append(fetch)
    copies = []
    for k, dst in enumerate((wg, wu, wd)):
        copy = pltpu.make_async_copy(w_ref.at[:, :, k], dst, sems.at[k])
        copy.start()
        copies.append(copy)
    is_first, half, core = at_ref[3], at_ref[4], at_ref[6]
    block = at_ref[5]
    rows = HALO + 512
    at_x = block // 2
    sides = ((core, attn_own, keep_ref), (1 - core, attn_other, send_ref))
    for c, attn, _ in sides:
        for x in range(4):
            af[:, pl.ds(pl.multiple_of(128 * (2 * x + c), 128), 128)] = attn[x]
    a = af[...]
    square = jnp.zeros((rows, 1), F32)
    for side, (c, _, _) in enumerate(sides):
        for i, back in enumerate((0, 1, 3, 2)):
            fetches[4 * side + i].wait()
            x = jnp.where(at_x >= back, at_x - back, at_x - back + 4)
            cols = pl.ds(pl.multiple_of(256 * (2 * x + c), 256), 256)
            branch = jnp.dot(a, wide_in[side, i, 0:1024, :], preferred_element_type=F32)
            m = (branch + wide_in[side, i, 1024:1024 + rows, :].astype(F32)).astype(BF16)
            if side == 0 and i == 0:
                mid[...] = m
            m = m.astype(F32)
            square = square + jnp.sum(m * m, axis=1, keepdims=True)
            scaled[:, cols] = (m * gain_ref[:, cols]).astype(BF16)
    inverse = lax.rsqrt(square * (1.0 / 2048) + NORM_EPS)
    mid_out_ref[...] = mid[pl.ds(pl.multiple_of(HALO + 256 * half, 16), 256), :]
    n = scaled[...]
    copies[0].wait()
    copies[1].wait()
    row = lax.broadcasted_iota(jnp.int32, (rows, 1), 0)
    keep = jnp.logical_not((row < HALO) & (is_first == 1))

    def mixed(weight, index):
        pre = jnp.dot(n, weight[...].reshape(2048, 352), preferred_element_type=F32)
        pre = (pre * inverse).astype(BF16).astype(F32)
        pre = jnp.where(keep, pre, 0.0)
        total = jnp.zeros((512, 352), F32)
        for k in range(3):
            total = total + conv_ref[2 * k + index:2 * k + index + 1, :] * pre[HALO - 2 + k:HALO - 2 + k + 512]
        return total

    gate = mixed(wg, 0)
    up = mixed(wu, 1)
    hidden = (gate / (1.0 + jnp.exp(-gate)) * up).astype(BF16)
    copies[2].wait()
    for c, _, part_ref in sides:
        for x in range(4):
            down = wd[pl.ds(2 * (2 * x + c), 2)].reshape(256, 352)
            part = lax.dot_general(hidden, down, (((1,), (1,)), ((), ())), preferred_element_type=F32).astype(BF16)
            for p in range(2):
                part_ref[p, x] = part[256 * p:256 * (p + 1)]


def feed(at, attn, other_attn, wide, other_wide, gain, conv, weights):
    smem = pl.BlockSpec(memory_space=pltpu.SMEM)
    vmem = pl.BlockSpec(memory_space=pltpu.VMEM)
    rows = HALO + 512
    half = jax.ShapeDtypeStruct((2, 4, 256, 256), BF16)
    hbm = pl.BlockSpec(memory_space=pltpu.HBM)
    return pl.pallas_call(
        feed_kernel,
        out_shape=(half, half, jax.ShapeDtypeStruct((256, 256), BF16)),
        in_specs=[smem, vmem, vmem, hbm, hbm, vmem, vmem, hbm],
        out_specs=(vmem, vmem, vmem),
        scratch_shapes=[
            pltpu.VMEM((rows, 1024), BF16),
            pltpu.VMEM((rows, 256), BF16),
            pltpu.VMEM((rows, 2048), BF16),
            pltpu.VMEM((2, 4, 1024 + rows, 256), BF16),
            pltpu.VMEM((16, 4, 32, 352), BF16),
            pltpu.VMEM((16, 4, 32, 352), BF16),
            pltpu.VMEM((16, 4, 32, 352), BF16),
            pltpu.SemaphoreType.DMA((11,)),
        ],
        compiler_params=pltpu.CompilerParams(vmem_limit_bytes=50 * 2**20),
        cost_estimate=pl.CostEstimate(flops=5 * 10**9, bytes_accessed=2**24, transcendentals=2 * 10**5),
        name="feed",
    )(at, attn, other_attn, wide, other_wide, gain, conv, weights)


def prepare_kernel(kv_ref, decay_ref, gate_ref, up_ref, down_ref, q_ref, resid_ref, keys_ref, halves_ref, tail_ref):
    turned = kv_ref[0].astype(F32).T.astype(BF16)
    row = lax.broadcasted_iota(jnp.int32, (8, 256), 0)
    value = jnp.where(row < 3, decay_ref[0:1, :], decay_ref[1:2, :])
    which = jnp.where(row < 3, row, row - 3)
    high, middle, low = split3(value)
    pick = jnp.where(which == 0, high.astype(F32), jnp.where(which == 1, middle.astype(F32), low.astype(F32)))
    gates = jnp.where(row < 6, pick, 0.0).astype(BF16)
    for i in range(4):
        keys_ref[i, 0:64, :] = turned[0:64]
        keys_ref[i, 64:72, :] = gates
        keys_ref[i, 72:136, :] = turned[64:128]
    for k, ref in enumerate((gate_ref, up_ref, down_ref)):
        value = ref[...].astype(F32)
        for p in range(2):
            piece = value[:, 352 * p:352 * (p + 1)].astype(BF16)
            for i in range(2):
                halves_ref[2 * i + p, k] = piece
    tail_ref[:, 0:128] = q_ref[256 - HALO:256, :]
    tail_ref[:, 128:384] = resid_ref[256 - HALO:256, :]


def prepare(*operands):
    vmem = pl.BlockSpec(memory_space=pltpu.VMEM)
    return pl.pallas_call(
        prepare_kernel,
        out_shape=(
            jax.ShapeDtypeStruct((4, 136, 256), BF16),
            jax.ShapeDtypeStruct((4, 3, 32, 352), BF16),
            jax.ShapeDtypeStruct((HALO, 384), BF16),
        ),
        in_specs=[vmem] * len(operands),
        out_specs=(vmem, vmem, vmem),
        cost_estimate=pl.CostEstimate(flops=10**7, bytes_accessed=2**20, transcendentals=0),
        name="prepare",
    )(*operands)


def layer(resid, queries, keys_values, cum_gate, out_weight, norm_gain, gate_weight, up_weight, conv_kernel, down_weight):
    zh, zl = lax.axis_index("zh"), lax.axis_index("zl")
    y, half = lax.axis_index(Y), lax.axis_index("yl")
    is_first = (lax.axis_index(SP) < 2).astype(jnp.int32)
    at = jnp.stack([zh, zl, y, is_first, half, lax.axis_index(TP), lax.axis_index("c")]).astype(jnp.int32)

    keys, halves, tail = prepare(
        keys_values, cum_gate, gate_weight, up_weight, down_weight.T, queries, resid
    )
    before = shifted(tail, SP, 1)
    rows_y = exchanged(halves, Y)
    weights = lax.all_gather(rows_y, Z, axis=0, tiled=False)
    mine = jnp.concatenate([before[:, 128:], resid], axis=0)
    theirs = shifted(mine, "yl", 1)
    own = exchanged(keys, "zh")
    low = jnp.concatenate([out_weight, mine, theirs[HALO:]], axis=0)
    high = jnp.concatenate([out_weight, theirs, mine[HALO:]], axis=0)
    wide = jnp.where(half == 0, low, high)
    wides = [wide] + [shifted(wide, "x", by) for by in (1, 3, 2)]
    last = shifted(own, Z, 1)
    nxt = shifted(own, Z, -1)
    far_a = shifted(own[:2], Z, -2)
    far_b = shifted(own[2:], Z, 2)
    group_q = spread(jnp.concatenate([before[:, :128], queries], axis=0), Y)

    queries, state = attend_own(at, cum_gate[:, 0], group_q, own)
    partial = attend_rest(at, cum_gate[:, 0], queries, state, nxt, far_a, far_b, last)
    partial = exchanged(partial, Y)
    wide = jnp.stack(wides)
    other_wide = shifted(wide, "c", 1)
    attn = merge(partial)
    attn = lax.all_gather(attn, "x", axis=0, tiled=False)
    other_attn = shifted(attn, "c", 1)
    conv = lax.dynamic_slice_in_dim(conv_kernel.reshape(6, 704), half * 352, 352, 1)
    keep, send, middle = feed(
        at, attn, other_attn, wide, other_wide, norm_gain.reshape(1, 2048), conv, weights
    )
    got = shifted(send, "c", 1)
    chip = (keep.astype(F32) + got.astype(F32)).astype(BF16).reshape(8, 256, 256)
    pieces = exchanged(chip, ("yl", "x"))
    total = jnp.sum(pieces.astype(F32), axis=0)
    return (middle.astype(F32) + total).astype(BF16)


def solution(mesh):
    finer = Mesh(mesh.devices.reshape(4, 4, 2, 2, 4, 2), SP + TP)
    return jax.shard_map(
        layer,
        mesh=finer,
        in_specs=(
            P(SP, TP),
            P(SP, TP),
            P(TP, SP, None),
            P(TP, SP),
            P(None, TP),
            P(),
            P(SP, TP),
            P(SP, TP),
            P(None, None, TP),
            P(TP, SP),
        ),
        out_specs=P(SP, TP),
        check_vma=False,
    )
```

```python
import functools

import jax
import jax.numpy as jnp
from jax import lax
from jax.experimental import pallas as pl
from jax.experimental.pallas import tpu as pltpu
from jax.sharding import Mesh
from jax.sharding import PartitionSpec as P


Z = ("zh", "zl")
Y = ("yh", "yl")
SP = Z + Y
TP = ("x", "c")
NORM_EPS = 1e-06
HALO = 16
MASKED = -1e30
F32 = jnp.float32
BF16 = jnp.bfloat16


def shifted(value, axis, by):
    size = lax.axis_size(axis)
    return lax.ppermute(value, axis, [(i, (i + by) % size) for i in range(size)])


def exchanged(value, axis):
    return lax.all_to_all(value, axis, 0, 0, tiled=True)


def split3(value):
    high = value.astype(BF16)
    rest = value - high.astype(F32)
    middle = rest.astype(BF16)
    low = (rest - middle.astype(F32)).astype(BF16)
    return high, middle, low


def put_keys(ka, va, chunk, d, piece, gate_ref):
    cols = pl.ds(256 * d, 256)
    row = lax.broadcasted_iota(jnp.int32, (8, 256), 0)
    ka[chunk, 0:64, cols] = piece[0:64, :]
    g = piece[64:72, :].astype(F32)
    bias = []
    for head in range(2):
        total = g[3 * head:3 * head + 1, :] + g[3 * head + 1:3 * head + 2, :]
        bias.append(gate_ref[head] - (total + g[3 * head + 2:3 * head + 3, :]))
    b = jnp.where(row < 3, bias[0], bias[1])
    which = jnp.where(row < 3, row, row - 3)
    high, middle, low = split3(b)
    pick = jnp.where(which == 0, high.astype(F32), jnp.where(which == 1, middle.astype(F32), low.astype(F32)))
    ka[chunk, 64:72, cols] = jnp.where(row < 6, pick, 0.0).astype(BF16)
    ka[chunk, 72:128, cols] = jnp.zeros((56, 256), BF16)
    va[chunk, 0:64, cols] = piece[72:136, :]
    va[chunk, 64:128, cols] = jnp.ones((64, 256), BF16)


def fold_keys(queries, keys, values, state, query_pos, key_pos):
    scores = []
    for i, q in enumerate(queries):
        s = lax.dot_general(q, keys, (((1,), (0,)), ((), ())), preferred_element_type=F32)
        if key_pos is not None:
            s = jnp.where(query_pos[i] >= key_pos, s, MASKED)
        scores.append(s)
    new_state = []
    for s, (top, acc) in zip(scores, state):
        new_top = jnp.maximum(top, jnp.max(s, axis=1, keepdims=True))
        p = jnp.exp(s - new_top).astype(BF16)
        more = lax.dot_general(p, values, (((1,), (1,)), ((), ())), preferred_element_type=F32)
        new_state.append((new_top, acc * jnp.exp(top - new_top) + more))
    return tuple(new_state)


def row_blocks(z):
    rows, part = HALO + 1024, 416
    blocks = []
    for start in range(0, 2 * rows, part):
        row = start + lax.broadcasted_iota(jnp.int32, (part, 1), 0)
        blocks.append((start, row >= rows, z * 1024 - HALO + jnp.where(row >= rows, row - rows, row)))
    return part, blocks


def attend_own_kernel(at_ref, gate_ref, q0_ref, q1_ref, q2_ref, q3_ref, own_ref, qa, state_ref, ka, va):
    q_refs = (q0_ref, q1_ref, q2_ref, q3_ref)
    zh, zl, y = at_ref[0], at_ref[1], at_ref[2]
    z = 4 * zh + zl
    rows = HALO + 1024
    lane = lax.broadcasted_iota(jnp.int32, (1, 128), 1)

    def put_queries(start, piece):
        x = piece.astype(F32) * 0.125
        for head in range(2):
            side = x if head == 0 else pltpu.roll(x, 64, 1)
            first = 64 + 3 * head
            ones = jnp.where((lane >= first) & (lane < first + 3), 1.0, 0.0)
            both = jnp.where(lane < 64, side, ones)
            first_row = pl.multiple_of(head * rows + start, HALO)
            qa[pl.ds(first_row, piece.shape[0]), :] = both.astype(BF16)

    for back, q_ref in zip((0, 1, 3, 2), q_refs):
        from_y = jnp.where(y >= back, y - back, y - back + 4)
        put_queries(HALO + 256 * from_y, q_ref[HALO:HALO + 256, :])

        @pl.when(from_y == 0)
        def _(q_ref=q_ref):
            put_queries(0, q_ref[0:HALO, :])

    for chunk in range(4):
        put_keys(ka, va, 0, chunk, own_ref[chunk], gate_ref)
    key_lane = lax.broadcasted_iota(jnp.int32, (1, 1024), 1)
    key_chunk = key_lane // 256
    key_pos = (4 * key_chunk + zl) * 1024 + y * 256 + (key_lane - 256 * key_chunk)
    part, blocks = row_blocks(z)
    state = tuple((jnp.full((part, 1), MASKED, F32), jnp.zeros((part, 128), F32)) for _ in blocks)
    queries = [qa[start:start + part, :] for start, _, _ in blocks]
    state = fold_keys(queries, ka[0], va[0], state, [pos for _, _, pos in blocks], key_pos)
    for (start, _, _), (top, acc) in zip(blocks, state):
        state_ref[start:start + part, :] = jnp.where(lane < 96, acc, top)


def attend_own(at, gate, queries, own):
    rows = HALO + 1024
    smem = pl.BlockSpec(memory_space=pltpu.SMEM)
    vmem = pl.BlockSpec(memory_space=pltpu.VMEM)
    return pl.pallas_call(
        attend_own_kernel,
        out_shape=(jax.ShapeDtypeStruct((2 * rows, 128), BF16), jax.ShapeDtypeStruct((2 * rows, 128), F32)),
        in_specs=[smem, smem] + [vmem] * 5,
        out_specs=(vmem, vmem),
        scratch_shapes=[pltpu.VMEM((1, 128, 1024), BF16), pltpu.VMEM((1, 128, 1024), BF16)],
        compiler_params=pltpu.CompilerParams(vmem_limit_bytes=30 * 2**20),
        cost_estimate=pl.CostEstimate(flops=2 * 10**9, bytes_accessed=2**20, transcendentals=2 * 10**6),
        name="attend_own",
    )(at, gate, *queries, own)


def attend_rest_kernel(at_ref, gate_ref, qa, state_ref, next_ref, far_a_ref, far_b_ref, last_ref,
                       out_ref, ka, va, states, norm_out, lse_rows, lse_dense):
    zh, zl, y = at_ref[0], at_ref[1], at_ref[2]
    z = 4 * zh + zl
    rows = HALO + 1024
    lane = lax.broadcasted_iota(jnp.int32, (1, 128), 1)
    for chunk in range(4):
        far = far_a_ref[chunk] if chunk < 2 else far_b_ref[chunk - 2]
        for d, piece in enumerate((next_ref[chunk], far, last_ref[chunk])):
            put_keys(ka, va, chunk, d, piece, gate_ref)
    key_lane = lax.broadcasted_iota(jnp.int32, (1, 768), 1)
    key_d = key_lane // 256
    turn = zl + 1 + key_d
    turn = jnp.where(turn >= 4, turn - 4, turn)
    key_rest = turn * 1024 + y * 256 + (key_lane - 256 * key_d)
    first_masked = jnp.maximum(zh - jnp.where(zl == 0, 1, 0), 0)
    part, blocks = row_blocks(z)

    for chunk in range(1, 4):
        @pl.when(chunk > zh)
        def _(chunk=chunk):
            states[chunk] = jnp.where(lane < 96, jnp.zeros((2 * rows, 128), F32), MASKED)

    def step(masked, chunk, _):
        fresh = tuple((jnp.full((part, 1), MASKED, F32), jnp.zeros((part, 128), F32)) for _ in blocks)
        queries = [qa[start:start + part, :] for start, _, _ in blocks]
        key_pos = chunk * 4096 + key_rest if masked else None
        state = fold_keys(queries, ka[chunk], va[chunk], fresh, [pos for _, _, pos in blocks], key_pos)
        for (start, _, _), (top, acc) in zip(blocks, state):
            states[chunk, start:start + part, :] = jnp.where(lane < 96, acc, top)
        return 0

    lax.fori_loop(0, first_masked, functools.partial(step, False), 0)
    lax.fori_loop(first_masked, zh + 1, functools.partial(step, True), 0)
    for start, second, _ in blocks:
        pieces = [state_ref[start:start + part, :]] + [states[chunk, start:start + part, :] for chunk in range(4)]
        tops = [piece[:, 127:128] for piece in pieces]
        top = functools.reduce(jnp.maximum, tops)
        acc = jnp.zeros((part, 128), F32)
        for piece, own_top in zip(pieces, tops):
            acc = acc + piece * jnp.exp(own_top - top)
        total = acc[:, 64:65]
        gate = jnp.where(second, gate_ref[1], gate_ref[0])
        norm_out[start:start + part, :] = acc * (1.0 / total)
        lse_rows[start:start + part, :] = jnp.broadcast_to(top + jnp.log(total) - gate, (part, 128))
    tail = lse_rows.shape[0] - 2 * rows
    lse_rows[pl.ds(2 * rows, tail), :] = jnp.zeros((tail, 128), F32)
    lse_dense[...] = jnp.zeros(lse_dense.shape, F32)
    diagonal = lax.broadcasted_iota(jnp.int32, (128, 128), 0) == lax.broadcasted_iota(jnp.int32, (128, 128), 1)
    pair_rows = HALO + 512
    for pair in range(2):
        a = norm_out[pl.ds(512 * pair, pair_rows), :]
        b = norm_out[pl.ds(rows + 512 * pair, pair_rows), :]
        joined = jnp.where(lane < 64, a, pltpu.roll(b, 64, 1)).astype(BF16)
        for head in range(2):
            for t in range(5):
                tile = lse_rows[pl.ds(head * rows + 512 * pair + 128 * t, 128), :]
                lse_dense[pl.ds(5 * head + t, 1), :] = jnp.sum(jnp.where(diagonal, tile, 0.0), axis=0, keepdims=True)
        parts = split3(lse_dense[...])
        for i in range(2):
            out_ref[2 * pair + i, 0:pair_rows, :] = joined
            for k in range(3):
                out_ref[2 * pair + i, pair_rows + 16 * k:pair_rows + 16 * (k + 1), :] = parts[k]


def attend_rest(at, gate, queries, state, nxt, far_a, far_b, last):
    rows = HALO + 1024
    pair_rows = HALO + 512
    smem = pl.BlockSpec(memory_space=pltpu.SMEM)
    vmem = pl.BlockSpec(memory_space=pltpu.VMEM)
    return pl.pallas_call(
        attend_rest_kernel,
        out_shape=jax.ShapeDtypeStruct((4, pair_rows + 48, 128), BF16),
        in_specs=[smem, smem] + [vmem] * 6,
        out_specs=vmem,
        scratch_shapes=[
            pltpu.VMEM((4, 128, 768), BF16),
            pltpu.VMEM((4, 128, 768), BF16),
            pltpu.VMEM((4, 2 * rows, 128), F32),
            pltpu.VMEM((2 * rows, 128), F32),
            pltpu.VMEM((2 * rows + 112, 128), F32),
            pltpu.VMEM((16, 128), F32),
        ],
        compiler_params=pltpu.CompilerParams(vmem_limit_bytes=36 * 2**20),
        cost_estimate=pl.CostEstimate(flops=6 * 10**9, bytes_accessed=4 * 2**20, transcendentals=6 * 10**6),
        name="attend_rest",
    )(at, gate, queries, state, nxt, far_a, far_b, last)


def merge_kernel(in_ref, out_ref):
    pair_rows = HALO + 512
    logs = []
    for i in range(4):
        parts = [in_ref[i, pair_rows + 16 * k:pair_rows + 16 * (k + 1), :].astype(F32) for k in range(3)]
        logs.append(parts[0] + parts[1] + parts[2])
    top = jnp.maximum(jnp.maximum(logs[0], logs[1]), jnp.maximum(logs[2], logs[3]))
    weights = [jnp.exp(v - top) for v in logs]
    total = weights[0] + weights[1] + weights[2] + weights[3]
    shares = [w / total for w in weights]
    lane = lax.broadcasted_iota(jnp.int32, (1, 128), 1)
    for t in range(5):
        size = 128 if t < 4 else pair_rows - 512
        diagonal = lax.broadcasted_iota(jnp.int32, (size, 128), 0) == lax.broadcasted_iota(jnp.int32, (size, 128), 1)
        acc = jnp.zeros((size, 128), F32)
        for i in range(4):
            cols = [
                jnp.sum(jnp.where(diagonal, shares[i][5 * head + t:5 * head + t + 1, :], 0.0), axis=1, keepdims=True)
                for head in range(2)
            ]
            share = jnp.where(lane < 64, cols[0], cols[1])
            acc = acc + share * in_ref[i, 128 * t:128 * t + size, :].astype(F32)
        out_ref[128 * t:128 * t + size, :] = acc.astype(BF16)


def merge(pieces):
    vmem = pl.BlockSpec(memory_space=pltpu.VMEM)
    return pl.pallas_call(
        merge_kernel,
        out_shape=jax.ShapeDtypeStruct((HALO + 512, 128), BF16),
        in_specs=[vmem],
        out_specs=vmem,
        compiler_params=pltpu.CompilerParams(vmem_limit_bytes=8 * 2**20),
        cost_estimate=pl.CostEstimate(flops=10**8, bytes_accessed=2**20, transcendentals=10**4),
        name="merge",
    )(pieces)


def feed_kernel(at_ref, attn_own, attn_other, wide_own, wide_other, gain_ref, conv_ref, w_ref,
                keep_ref, send_ref, mid_out_ref, af, mid, scaled, wide_in, wg, wu, wd, sems):
    fetches = [
        pltpu.make_async_copy(wide.at[i], wide_in.at[side, i], sems.at[3 + 4 * side + i])
        for side, wide in enumerate((wide_own, wide_other))
        for i in range(4)
    ]
    copies = [pltpu.make_async_copy(w_ref.at[:, :, k], dst, sems.at[k]) for k, dst in enumerate((wg, wu, wd))]
    for fetch in fetches + copies:
        fetch.start()
    is_first, half, core = at_ref[3], at_ref[4], at_ref[6]
    block = at_ref[5]
    rows = HALO + 512
    at_x = block // 2
    sides = ((core, attn_own, keep_ref), (1 - core, attn_other, send_ref))
    for c, attn, _ in sides:
        for x in range(4):
            af[:, pl.ds(pl.multiple_of(128 * (2 * x + c), 128), 128)] = attn[x]
    a = af[...]
    square = jnp.zeros((rows, 128), F32)
    for side, (c, _, _) in enumerate(sides):
        for i, back in enumerate((0, 1, 3, 2)):
            fetches[4 * side + i].wait()
            x = jnp.where(at_x >= back, at_x - back, at_x - back + 4)
            cols = pl.ds(pl.multiple_of(256 * (2 * x + c), 256), 256)
            branch = jnp.dot(a, wide_in[side, i, 0:1024, :], preferred_element_type=F32)
            m = (branch + wide_in[side, i, 1024:1024 + rows, :].astype(F32)).astype(BF16)
            if side == 0 and i == 0:
                mid[...] = m
            m = m.astype(F32)
            squared = m * m
            square = square + squared[:, :128] + squared[:, 128:]
            scaled[:, cols] = (m * gain_ref[:, cols]).astype(BF16)
    inverse = lax.rsqrt(jnp.sum(square, axis=1, keepdims=True) * (1.0 / 2048) + NORM_EPS)
    mid_out_ref[...] = mid[pl.ds(pl.multiple_of(HALO + 256 * half, 16), 256), :]
    n = scaled[...]
    copies[0].wait()
    copies[1].wait()
    row = lax.broadcasted_iota(jnp.int32, (rows, 1), 0)
    keep = jnp.logical_not((row < HALO) & (is_first == 1))

    def projected(weight):
        pre = jnp.dot(n, weight[...].reshape(2048, 352), preferred_element_type=F32)
        return jnp.where(keep, (pre * inverse).astype(BF16).astype(F32), 0.0)

    def mixed(pre, index, start):
        total = jnp.zeros((256, 352), F32)
        for k in range(3):
            first = HALO - 2 + k + start
            total = total + conv_ref[2 * k + index:2 * k + index + 1, :] * pre[first:first + 256]
        return total

    pre_gate = projected(wg)
    pre_up = projected(wu)
    copies[2].wait()
    for p in range(2):
        gate = mixed(pre_gate, 0, 256 * p)
        hidden = (gate / (1.0 + jnp.exp(-gate)) * mixed(pre_up, 1, 256 * p)).astype(BF16)
        for c, _, part_ref in sides:
            for x in range(4):
                down = wd[pl.ds(2 * (2 * x + c), 2)].reshape(256, 352)
                part = lax.dot_general(hidden, down, (((1,), (1,)), ((), ())), preferred_element_type=F32)
                part_ref[p, x] = part.astype(BF16)


def feed(at, attn, other_attn, wide, other_wide, gain, conv, weights):
    smem = pl.BlockSpec(memory_space=pltpu.SMEM)
    vmem = pl.BlockSpec(memory_space=pltpu.VMEM)
    rows = HALO + 512
    half = jax.ShapeDtypeStruct((2, 4, 256, 256), BF16)
    hbm = pl.BlockSpec(memory_space=pltpu.HBM)
    return pl.pallas_call(
        feed_kernel,
        out_shape=(half, half, jax.ShapeDtypeStruct((256, 256), BF16)),
        in_specs=[smem, vmem, vmem, hbm, hbm, vmem, vmem, hbm],
        out_specs=(vmem, vmem, vmem),
        scratch_shapes=[
            pltpu.VMEM((rows, 1024), BF16),
            pltpu.VMEM((rows, 256), BF16),
            pltpu.VMEM((rows, 2048), BF16),
            pltpu.VMEM((2, 4, 1024 + rows, 256), BF16),
            pltpu.VMEM((16, 4, 32, 352), BF16),
            pltpu.VMEM((16, 4, 32, 352), BF16),
            pltpu.VMEM((16, 4, 32, 352), BF16),
            pltpu.SemaphoreType.DMA((11,)),
        ],
        compiler_params=pltpu.CompilerParams(vmem_limit_bytes=50 * 2**20),
        cost_estimate=pl.CostEstimate(flops=5 * 10**9, bytes_accessed=2**24, transcendentals=2 * 10**5),
        name="feed",
    )(at, attn, other_attn, wide, other_wide, gain, conv, weights)


def prepare_kernel(kv_ref, decay_ref, gate_ref, up_ref, down_ref, q_ref, resid_ref, keys_ref, halves_ref, tail_ref):
    turned = kv_ref[0].astype(F32).T.astype(BF16)
    row = lax.broadcasted_iota(jnp.int32, (8, 256), 0)
    value = jnp.where(row < 3, decay_ref[0:1, :], decay_ref[1:2, :])
    which = jnp.where(row < 3, row, row - 3)
    high, middle, low = split3(value)
    pick = jnp.where(which == 0, high.astype(F32), jnp.where(which == 1, middle.astype(F32), low.astype(F32)))
    gates = jnp.where(row < 6, pick, 0.0).astype(BF16)
    for i in range(4):
        keys_ref[i, 0:64, :] = turned[0:64]
        keys_ref[i, 64:72, :] = gates
        keys_ref[i, 72:136, :] = turned[64:128]
    for k, ref in enumerate((gate_ref, up_ref, down_ref)):
        value = ref[...].astype(F32)
        for p in range(2):
            piece = value[:, 352 * p:352 * (p + 1)].astype(BF16)
            for i in range(2):
                halves_ref[2 * i + p, k] = piece
    tail_ref[:, 0:128] = q_ref[256 - HALO:256, :]
    tail_ref[:, 128:384] = resid_ref[256 - HALO:256, :]


def prepare(*operands):
    vmem = pl.BlockSpec(memory_space=pltpu.VMEM)
    return pl.pallas_call(
        prepare_kernel,
        out_shape=(
            jax.ShapeDtypeStruct((4, 136, 256), BF16),
            jax.ShapeDtypeStruct((4, 3, 32, 352), BF16),
            jax.ShapeDtypeStruct((HALO, 384), BF16),
        ),
        in_specs=[vmem] * len(operands),
        out_specs=(vmem, vmem, vmem),
        cost_estimate=pl.CostEstimate(flops=10**7, bytes_accessed=2**20, transcendentals=0),
        name="prepare",
    )(*operands)


def layer(resid, queries, keys_values, cum_gate, out_weight, norm_gain, gate_weight, up_weight, conv_kernel, down_weight):
    zh, zl = lax.axis_index("zh"), lax.axis_index("zl")
    y, half = lax.axis_index(Y), lax.axis_index("yl")
    is_first = (lax.axis_index(SP) < 2).astype(jnp.int32)
    at = jnp.stack([zh, zl, y, is_first, half, lax.axis_index(TP), lax.axis_index("c")]).astype(jnp.int32)

    keys, halves, tail = prepare(
        keys_values, cum_gate, gate_weight, up_weight, down_weight.T, queries, resid
    )
    before = shifted(tail, SP, 1)
    rows_y = exchanged(halves, Y)
    weights = lax.all_gather(rows_y, Z, axis=0, tiled=False)
    mine = jnp.concatenate([before[:, 128:], resid], axis=0)
    theirs = shifted(mine, "yl", 1)
    own = exchanged(keys, "zh")
    low = jnp.concatenate([out_weight, mine, theirs[HALO:]], axis=0)
    high = jnp.concatenate([out_weight, theirs, mine[HALO:]], axis=0)
    wide = jnp.where(half == 0, low, high)
    wides = [wide] + [shifted(wide, "x", by) for by in (1, 3, 2)]
    last = shifted(own, Z, 1)
    nxt = shifted(own, Z, -1)
    far_a = shifted(own[:2], Z, -2)
    far_b = shifted(own[2:], Z, 2)
    queries = jnp.concatenate([before[:, :128], queries], axis=0)
    group_q = [queries] + [shifted(queries, Y, by) for by in (1, 3, 2)]

    queries, state = attend_own(at, cum_gate[:, 0], group_q, own)
    partial = attend_rest(at, cum_gate[:, 0], queries, state, nxt, far_a, far_b, last)
    partial = exchanged(partial, Y)
    wide = jnp.stack(wides)
    other_wide = shifted(wide, "c", 1)
    attn = merge(partial)
    attn = lax.all_gather(attn, "x", axis=0, tiled=False)
    other_attn = shifted(attn, "c", 1)
    conv = lax.dynamic_slice_in_dim(conv_kernel.reshape(6, 704), half * 352, 352, 1)
    keep, send, middle = feed(
        at, attn, other_attn, wide, other_wide, norm_gain.reshape(1, 2048), conv, weights
    )
    got = shifted(send, "c", 1)
    chip = (keep.astype(F32) + got.astype(F32)).astype(BF16).reshape(8, 256, 256)
    pieces = exchanged(chip, ("yl", "x"))
    total = jnp.sum(pieces.astype(F32), axis=0)
    return (middle.astype(F32) + total).astype(BF16)


def solution(mesh):
    finer = Mesh(mesh.devices.reshape(4, 4, 2, 2, 4, 2), SP + TP)
    return jax.shard_map(
        layer,
        mesh=finer,
        in_specs=(
            P(SP, TP),
            P(SP, TP),
            P(TP, SP, None),
            P(TP, SP),
            P(None, TP),
            P(),
            P(SP, TP),
            P(SP, TP),
            P(None, None, TP),
            P(TP, SP),
        ),
        out_specs=P(SP, TP),
        check_vma=False,
    )
```

```python
import functools

import jax
import jax.numpy as jnp
from jax import lax
from jax.experimental import pallas as pl
from jax.experimental.pallas import tpu as pltpu
from jax.sharding import Mesh
from jax.sharding import PartitionSpec as P


Z = ("zh", "zl")
Y = ("yh", "yl")
SP = Z + Y
TP = ("x", "c")
NORM_EPS = 1e-06
HALO = 16
MASKED = -1e30
F32 = jnp.float32
BF16 = jnp.bfloat16


def shifted(value, axis, by):
    size = lax.axis_size(axis)
    return lax.ppermute(value, axis, [(i, (i + by) % size) for i in range(size)])


def exchanged(value, axis):
    return lax.all_to_all(value, axis, 0, 0, tiled=True)


def spread(value, axis):
    size = lax.axis_size(axis)
    return exchanged(jnp.broadcast_to(value[None], (size, *value.shape)), axis)


def split3(value):
    high = value.astype(BF16)
    rest = value - high.astype(F32)
    middle = rest.astype(BF16)
    low = (rest - middle.astype(F32)).astype(BF16)
    return high, middle, low


def put_keys(ka, va, chunk, d, piece, gate_ref):
    cols = pl.ds(256 * d, 256)
    row = lax.broadcasted_iota(jnp.int32, (8, 256), 0)
    ka[chunk, 0:64, cols] = piece[0:64, :]
    g = piece[64:72, :].astype(F32)
    bias = []
    for head in range(2):
        total = g[3 * head:3 * head + 1, :] + g[3 * head + 1:3 * head + 2, :]
        bias.append(gate_ref[head] - (total + g[3 * head + 2:3 * head + 3, :]))
    b = jnp.where(row < 3, bias[0], bias[1])
    which = jnp.where(row < 3, row, row - 3)
    high, middle, low = split3(b)
    pick = jnp.where(which == 0, high.astype(F32), jnp.where(which == 1, middle.astype(F32), low.astype(F32)))
    ka[chunk, 64:72, cols] = jnp.where(row < 6, pick, 0.0).astype(BF16)
    ka[chunk, 72:128, cols] = jnp.zeros((56, 256), BF16)
    va[chunk, 0:64, cols] = piece[72:136, :]
    va[chunk, 64:128, cols] = jnp.ones((64, 256), BF16)


def fold_keys(queries, keys, values, state, query_pos, key_pos):
    scores = []
    for i, q in enumerate(queries):
        s = lax.dot_general(q, keys, (((1,), (0,)), ((), ())), preferred_element_type=F32)
        if key_pos is not None:
            s = jnp.where(query_pos[i] >= key_pos, s, MASKED)
        scores.append(s)
    new_state = []
    for s, (top, acc) in zip(scores, state):
        new_top = jnp.maximum(top, jnp.max(s, axis=1, keepdims=True))
        p = jnp.exp(s - new_top).astype(BF16)
        more = lax.dot_general(p, values, (((1,), (1,)), ((), ())), preferred_element_type=F32)
        new_state.append((new_top, acc * jnp.exp(top - new_top) + more))
    return tuple(new_state)


def row_blocks(z):
    rows, part = HALO + 1024, 416
    blocks = []
    for start in range(0, 2 * rows, part):
        row = start + lax.broadcasted_iota(jnp.int32, (part, 1), 0)
        blocks.append((start, row >= rows, z * 1024 - HALO + jnp.where(row >= rows, row - rows, row)))
    return part, blocks


def attend_own_kernel(at_ref, gate_ref, q_ref, own_ref, qa, state_ref, ka, va):
    zh, zl, y = at_ref[0], at_ref[1], at_ref[2]
    z = 4 * zh + zl
    rows = HALO + 1024
    lane = lax.broadcasted_iota(jnp.int32, (1, 128), 1)

    def put_queries(start, piece):
        x = piece.astype(F32) * 0.125
        for head in range(2):
            side = x if head == 0 else pltpu.roll(x, 64, 1)
            first = 64 + 3 * head
            ones = jnp.where((lane >= first) & (lane < first + 3), 1.0, 0.0)
            both = jnp.where(lane < 64, side, ones)
            qa[head * rows + start:head * rows + start + piece.shape[0], :] = both.astype(BF16)

    put_queries(0, q_ref[0, 0:HALO, :])
    for i in range(4):
        put_queries(HALO + 256 * i, q_ref[i, HALO:HALO + 256, :])
    for chunk in range(4):
        put_keys(ka, va, 0, chunk, own_ref[chunk], gate_ref)
    key_lane = lax.broadcasted_iota(jnp.int32, (1, 1024), 1)
    key_chunk = key_lane // 256
    key_pos = (4 * key_chunk + zl) * 1024 + y * 256 + (key_lane - 256 * key_chunk)
    part, blocks = row_blocks(z)
    state = tuple((jnp.full((part, 1), MASKED, F32), jnp.zeros((part, 128), F32)) for _ in blocks)
    queries = [qa[start:start + part, :] for start, _, _ in blocks]
    state = fold_keys(queries, ka[0], va[0], state, [pos for _, _, pos in blocks], key_pos)
    for (start, _, _), (top, acc) in zip(blocks, state):
        state_ref[start:start + part, :] = jnp.where(lane < 96, acc, top)


def attend_own(at, gate, queries, own):
    rows = HALO + 1024
    smem = pl.BlockSpec(memory_space=pltpu.SMEM)
    vmem = pl.BlockSpec(memory_space=pltpu.VMEM)
    return pl.pallas_call(
        attend_own_kernel,
        out_shape=(jax.ShapeDtypeStruct((2 * rows, 128), BF16), jax.ShapeDtypeStruct((2 * rows, 128), F32)),
        in_specs=[smem, smem, vmem, vmem],
        out_specs=(vmem, vmem),
        scratch_shapes=[pltpu.VMEM((1, 128, 1024), BF16), pltpu.VMEM((1, 128, 1024), BF16)],
        compiler_params=pltpu.CompilerParams(vmem_limit_bytes=30 * 2**20),
        cost_estimate=pl.CostEstimate(flops=2 * 10**9, bytes_accessed=2**20, transcendentals=2 * 10**6),
        name="attend_own",
    )(at, gate, queries, own)


def attend_rest_kernel(at_ref, gate_ref, qa, state_ref, next_ref, far_a_ref, far_b_ref, last_ref,
                       out_ref, ka, va, states, norm_out, lse_rows, lse_dense):
    zh, zl, y = at_ref[0], at_ref[1], at_ref[2]
    z = 4 * zh + zl
    rows = HALO + 1024
    lane = lax.broadcasted_iota(jnp.int32, (1, 128), 1)
    for chunk in range(4):
        far = far_a_ref[chunk] if chunk < 2 else far_b_ref[chunk - 2]
        for d, piece in enumerate((next_ref[chunk], far, last_ref[chunk])):
            put_keys(ka, va, chunk, d, piece, gate_ref)
    key_lane = lax.broadcasted_iota(jnp.int32, (1, 768), 1)
    key_d = key_lane // 256
    turn = zl + 1 + key_d
    turn = jnp.where(turn >= 4, turn - 4, turn)
    key_rest = turn * 1024 + y * 256 + (key_lane - 256 * key_d)
    first_masked = jnp.maximum(zh - jnp.where(zl == 0, 1, 0), 0)
    part, blocks = row_blocks(z)

    for chunk in range(1, 4):
        @pl.when(chunk > zh)
        def _(chunk=chunk):
            states[chunk] = jnp.where(lane < 96, jnp.zeros((2 * rows, 128), F32), MASKED)

    def step(masked, chunk, _):
        fresh = tuple((jnp.full((part, 1), MASKED, F32), jnp.zeros((part, 128), F32)) for _ in blocks)
        queries = [qa[start:start + part, :] for start, _, _ in blocks]
        key_pos = chunk * 4096 + key_rest if masked else None
        state = fold_keys(queries, ka[chunk], va[chunk], fresh, [pos for _, _, pos in blocks], key_pos)
        for (start, _, _), (top, acc) in zip(blocks, state):
            states[chunk, start:start + part, :] = jnp.where(lane < 96, acc, top)
        return 0

    lax.fori_loop(0, first_masked, functools.partial(step, False), 0)
    lax.fori_loop(first_masked, zh + 1, functools.partial(step, True), 0)
    for start, second, _ in blocks:
        pieces = [state_ref[start:start + part, :]] + [states[chunk, start:start + part, :] for chunk in range(4)]
        tops = [piece[:, 127:128] for piece in pieces]
        top = functools.reduce(jnp.maximum, tops)
        acc = jnp.zeros((part, 128), F32)
        for piece, own_top in zip(pieces, tops):
            acc = acc + piece * jnp.exp(own_top - top)
        total = acc[:, 64:65]
        gate = jnp.where(second, gate_ref[1], gate_ref[0])
        norm_out[start:start + part, :] = acc * (1.0 / total)
        lse_rows[start:start + part, :] = jnp.broadcast_to(top + jnp.log(total) - gate, (part, 128))
    tail = lse_rows.shape[0] - 2 * rows
    lse_rows[pl.ds(2 * rows, tail), :] = jnp.zeros((tail, 128), F32)
    lse_dense[...] = jnp.zeros(lse_dense.shape, F32)
    diagonal = lax.broadcasted_iota(jnp.int32, (128, 128), 0) == lax.broadcasted_iota(jnp.int32, (128, 128), 1)
    pair_rows = HALO + 512
    for pair in range(2):
        a = norm_out[pl.ds(512 * pair, pair_rows), :]
        b = norm_out[pl.ds(rows + 512 * pair, pair_rows), :]
        joined = jnp.where(lane < 64, a, pltpu.roll(b, 64, 1)).astype(BF16)
        for head in range(2):
            for t in range(5):
                tile = lse_rows[pl.ds(head * rows + 512 * pair + 128 * t, 128), :]
                lse_dense[pl.ds(5 * head + t, 1), :] = jnp.sum(jnp.where(diagonal, tile, 0.0), axis=0, keepdims=True)
        parts = split3(lse_dense[...])
        for i in range(2):
            out_ref[2 * pair + i, 0:pair_rows, :] = joined
            for k in range(3):
                out_ref[2 * pair + i, pair_rows + 16 * k:pair_rows + 16 * (k + 1), :] = parts[k]


def attend_rest(at, gate, queries, state, nxt, far_a, far_b, last):
    rows = HALO + 1024
    pair_rows = HALO + 512
    smem = pl.BlockSpec(memory_space=pltpu.SMEM)
    vmem = pl.BlockSpec(memory_space=pltpu.VMEM)
    return pl.pallas_call(
        attend_rest_kernel,
        out_shape=jax.ShapeDtypeStruct((4, pair_rows + 48, 128), BF16),
        in_specs=[smem, smem] + [vmem] * 6,
        out_specs=vmem,
        scratch_shapes=[
            pltpu.VMEM((4, 128, 768), BF16),
            pltpu.VMEM((4, 128, 768), BF16),
            pltpu.VMEM((4, 2 * rows, 128), F32),
            pltpu.VMEM((2 * rows, 128), F32),
            pltpu.VMEM((2 * rows + 112, 128), F32),
            pltpu.VMEM((16, 128), F32),
        ],
        compiler_params=pltpu.CompilerParams(vmem_limit_bytes=36 * 2**20),
        cost_estimate=pl.CostEstimate(flops=6 * 10**9, bytes_accessed=4 * 2**20, transcendentals=6 * 10**6),
        name="attend_rest",
    )(at, gate, queries, state, nxt, far_a, far_b, last)


def merge_kernel(in_ref, out_ref):
    pair_rows = HALO + 512
    logs = []
    for i in range(4):
        parts = [in_ref[i, pair_rows + 16 * k:pair_rows + 16 * (k + 1), :].astype(F32) for k in range(3)]
        logs.append(parts[0] + parts[1] + parts[2])
    top = jnp.maximum(jnp.maximum(logs[0], logs[1]), jnp.maximum(logs[2], logs[3]))
    weights = [jnp.exp(v - top) for v in logs]
    total = weights[0] + weights[1] + weights[2] + weights[3]
    shares = [w / total for w in weights]
    lane = lax.broadcasted_iota(jnp.int32, (1, 128), 1)
    for t in range(5):
        size = 128 if t < 4 else pair_rows - 512
        diagonal = lax.broadcasted_iota(jnp.int32, (size, 128), 0) == lax.broadcasted_iota(jnp.int32, (size, 128), 1)
        acc = jnp.zeros((size, 128), F32)
        for i in range(4):
            cols = [
                jnp.sum(jnp.where(diagonal, shares[i][5 * head + t:5 * head + t + 1, :], 0.0), axis=1, keepdims=True)
                for head in range(2)
            ]
            share = jnp.where(lane < 64, cols[0], cols[1])
            acc = acc + share * in_ref[i, 128 * t:128 * t + size, :].astype(F32)
        out_ref[128 * t:128 * t + size, :] = acc.astype(BF16)


def merge(pieces):
    vmem = pl.BlockSpec(memory_space=pltpu.VMEM)
    return pl.pallas_call(
        merge_kernel,
        out_shape=jax.ShapeDtypeStruct((HALO + 512, 128), BF16),
        in_specs=[vmem],
        out_specs=vmem,
        compiler_params=pltpu.CompilerParams(vmem_limit_bytes=8 * 2**20),
        cost_estimate=pl.CostEstimate(flops=10**8, bytes_accessed=2**20, transcendentals=10**4),
        name="merge",
    )(pieces)


def feed_kernel(at_ref, attn_own, attn_other, wide_own, wide_other, gain_ref, conv_ref, w_ref,
                keep_ref, send_ref, mid_out_ref, af, mid, scaled, wide_in, wg, wu, wd, sems):
    fetches = [
        pltpu.make_async_copy(wide.at[i], wide_in.at[side, i], sems.at[3 + 4 * side + i])
        for side, wide in enumerate((wide_own, wide_other))
        for i in range(4)
    ]
    copies = [pltpu.make_async_copy(w_ref.at[:, :, k], dst, sems.at[k]) for k, dst in enumerate((wg, wu, wd))]
    for fetch in fetches + copies:
        fetch.start()
    is_first, half, core = at_ref[3], at_ref[4], at_ref[6]
    block = at_ref[5]
    rows = HALO + 512
    at_x = block // 2
    sides = ((core, attn_own, keep_ref), (1 - core, attn_other, send_ref))
    for c, attn, _ in sides:
        for x in range(4):
            af[:, pl.ds(pl.multiple_of(128 * (2 * x + c), 128), 128)] = attn[x]
    a = af[...]
    square = jnp.zeros((rows, 128), F32)
    for side, (c, _, _) in enumerate(sides):
        for i, back in enumerate((0, 1, 3, 2)):
            fetches[4 * side + i].wait()
            x = jnp.where(at_x >= back, at_x - back, at_x - back + 4)
            cols = pl.ds(pl.multiple_of(256 * (2 * x + c), 256), 256)
            branch = jnp.dot(a, wide_in[side, i, 0:1024, :], preferred_element_type=F32)
            m = (branch + wide_in[side, i, 1024:1024 + rows, :].astype(F32)).astype(BF16)
            if side == 0 and i == 0:
                mid[...] = m
            m = m.astype(F32)
            squared = m * m
            square = square + squared[:, :128] + squared[:, 128:]
            scaled[:, cols] = (m * gain_ref[:, cols]).astype(BF16)
    inverse = lax.rsqrt(jnp.sum(square, axis=1, keepdims=True) * (1.0 / 2048) + NORM_EPS)
    mid_out_ref[...] = mid[pl.ds(pl.multiple_of(HALO + 256 * half, 16), 256), :]
    n = scaled[...]
    copies[0].wait()
    copies[1].wait()
    row = lax.broadcasted_iota(jnp.int32, (rows, 1), 0)
    keep = jnp.logical_not((row < HALO) & (is_first == 1))

    def projected(weight):
        pre = jnp.dot(n, weight[...].reshape(2048, 352), preferred_element_type=F32)
        return jnp.where(keep, (pre * inverse).astype(BF16).astype(F32), 0.0)

    def mixed(pre, index, start):
        total = jnp.zeros((256, 352), F32)
        for k in range(3):
            first = HALO - 2 + k + start
            total = total + conv_ref[2 * k + index:2 * k + index + 1, :] * pre[first:first + 256]
        return total

    pre_gate = projected(wg)
    pre_up = projected(wu)
    copies[2].wait()
    for p in range(2):
        gate = mixed(pre_gate, 0, 256 * p)
        hidden = (gate / (1.0 + jnp.exp(-gate)) * mixed(pre_up, 1, 256 * p)).astype(BF16)
        for c, _, part_ref in sides:
            for x in range(4):
                down = wd[pl.ds(2 * (2 * x + c), 2)].reshape(256, 352)
                part = lax.dot_general(hidden, down, (((1,), (1,)), ((), ())), preferred_element_type=F32)
                part_ref[p, x] = part.astype(BF16)


def feed(at, attn, other_attn, wide, other_wide, gain, conv, weights):
    smem = pl.BlockSpec(memory_space=pltpu.SMEM)
    vmem = pl.BlockSpec(memory_space=pltpu.VMEM)
    rows = HALO + 512
    half = jax.ShapeDtypeStruct((2, 4, 256, 256), BF16)
    hbm = pl.BlockSpec(memory_space=pltpu.HBM)
    return pl.pallas_call(
        feed_kernel,
        out_shape=(half, half, jax.ShapeDtypeStruct((256, 256), BF16)),
        in_specs=[smem, vmem, vmem, hbm, hbm, vmem, vmem, hbm],
        out_specs=(vmem, vmem, vmem),
        scratch_shapes=[
            pltpu.VMEM((rows, 1024), BF16),
            pltpu.VMEM((rows, 256), BF16),
            pltpu.VMEM((rows, 2048), BF16),
            pltpu.VMEM((2, 4, 1024 + rows, 256), BF16),
            pltpu.VMEM((16, 4, 32, 352), BF16),
            pltpu.VMEM((16, 4, 32, 352), BF16),
            pltpu.VMEM((16, 4, 32, 352), BF16),
            pltpu.SemaphoreType.DMA((11,)),
        ],
        compiler_params=pltpu.CompilerParams(vmem_limit_bytes=50 * 2**20),
        cost_estimate=pl.CostEstimate(flops=5 * 10**9, bytes_accessed=2**24, transcendentals=2 * 10**5),
        name="feed",
    )(at, attn, other_attn, wide, other_wide, gain, conv, weights)


def prepare_kernel(kv_ref, decay_ref, gate_ref, up_ref, down_ref, q_ref, resid_ref, keys_ref, halves_ref, tail_ref):
    turned = kv_ref[0].astype(F32).T.astype(BF16)
    row = lax.broadcasted_iota(jnp.int32, (8, 256), 0)
    value = jnp.where(row < 3, decay_ref[0:1, :], decay_ref[1:2, :])
    which = jnp.where(row < 3, row, row - 3)
    high, middle, low = split3(value)
    pick = jnp.where(which == 0, high.astype(F32), jnp.where(which == 1, middle.astype(F32), low.astype(F32)))
    gates = jnp.where(row < 6, pick, 0.0).astype(BF16)
    for i in range(4):
        keys_ref[i, 0:64, :] = turned[0:64]
        keys_ref[i, 64:72, :] = gates
        keys_ref[i, 72:136, :] = turned[64:128]
    for k, ref in enumerate((gate_ref, up_ref, down_ref)):
        value = ref[...].astype(F32)
        for p in range(2):
            piece = value[:, 352 * p:352 * (p + 1)].astype(BF16)
            for i in range(2):
                halves_ref[2 * i + p, k] = piece
    tail_ref[:, 0:128] = q_ref[256 - HALO:256, :]
    tail_ref[:, 128:384] = resid_ref[256 - HALO:256, :]


def prepare(*operands):
    vmem = pl.BlockSpec(memory_space=pltpu.VMEM)
    return pl.pallas_call(
        prepare_kernel,
        out_shape=(
            jax.ShapeDtypeStruct((4, 136, 256), BF16),
            jax.ShapeDtypeStruct((4, 3, 32, 352), BF16),
            jax.ShapeDtypeStruct((HALO, 384), BF16),
        ),
        in_specs=[vmem] * len(operands),
        out_specs=(vmem, vmem, vmem),
        cost_estimate=pl.CostEstimate(flops=10**7, bytes_accessed=2**20, transcendentals=0),
        name="prepare",
    )(*operands)


def layer(resid, queries, keys_values, cum_gate, out_weight, norm_gain, gate_weight, up_weight, conv_kernel, down_weight):
    zh, zl = lax.axis_index("zh"), lax.axis_index("zl")
    y, half = lax.axis_index(Y), lax.axis_index("yl")
    is_first = (lax.axis_index(SP) < 2).astype(jnp.int32)
    at = jnp.stack([zh, zl, y, is_first, half, lax.axis_index(TP), lax.axis_index("c")]).astype(jnp.int32)

    keys, halves, tail = prepare(
        keys_values, cum_gate, gate_weight, up_weight, down_weight.T, queries, resid
    )
    before = shifted(tail, SP, 1)
    rows_y = exchanged(halves, Y)
    weights = lax.all_gather(rows_y, Z, axis=0, tiled=False)
    mine = jnp.concatenate([before[:, 128:], resid], axis=0)
    theirs = shifted(mine, "yl", 1)
    own = exchanged(keys, "zh")
    low = jnp.concatenate([out_weight, mine, theirs[HALO:]], axis=0)
    high = jnp.concatenate([out_weight, theirs, mine[HALO:]], axis=0)
    wide = jnp.where(half == 0, low, high)
    wides = [wide, shifted(wide, "x", 1), shifted(wide, "x", 3)]
    wides.append(shifted(wide, "x", 2))
    last = shifted(own, Z, 1)
    nxt = shifted(own, Z, -1)
    far_a = shifted(own[:2], Z, -2)
    far_b = shifted(own[2:], Z, 2)
    group_q = spread(jnp.concatenate([before[:, :128], queries], axis=0), Y)

    queries, state = attend_own(at, cum_gate[:, 0], group_q, own)
    partial = attend_rest(at, cum_gate[:, 0], queries, state, nxt, far_a, far_b, last)
    partial = exchanged(partial, Y)
    wide = jnp.stack(wides)
    other_wide = shifted(wide, "c", 1)
    attn = merge(partial)
    attn = lax.all_gather(attn, "x", axis=0, tiled=False)
    other_attn = shifted(attn, "c", 1)
    conv = lax.dynamic_slice_in_dim(conv_kernel.reshape(6, 704), half * 352, 352, 1)
    keep, send, middle = feed(
        at, attn, other_attn, wide, other_wide, norm_gain.reshape(1, 2048), conv, weights
    )
    got = shifted(send, "c", 1)
    chip = (keep.astype(F32) + got.astype(F32)).astype(BF16).reshape(8, 256, 256)
    pieces = exchanged(chip, ("yl", "x"))
    total = jnp.sum(pieces.astype(F32), axis=0)
    return (middle.astype(F32) + total).astype(BF16)


def solution(mesh):
    finer = Mesh(mesh.devices.reshape(4, 4, 2, 2, 4, 2), SP + TP)
    return jax.shard_map(
        layer,
        mesh=finer,
        in_specs=(
            P(SP, TP),
            P(SP, TP),
            P(TP, SP, None),
            P(TP, SP),
            P(None, TP),
            P(),
            P(SP, TP),
            P(SP, TP),
            P(None, None, TP),
            P(TP, SP),
        ),
        out_specs=P(SP, TP),
        check_vma=False,
    )
```
